512 devices in a mesh: ep: 32 (over z, core), tp: 16 (over y, x).
Axes of the slice: x: 4, y: 4, z: 16, core: 2. Of those that a mesh axis runs over, the one named last changes fastest.
Arguments:
- mixer_rows: bfloat16 [16384, 2048], P('ep', 'tp'), may hold values from -6 to 6
- expert_rows: bfloat16 [16384, 2048], P('ep', 'tp'), may hold values from -6 to 6
- mixer_gain: float32 [2048], replicated, may hold values from 0.1 to 1.9
- pool_scale: float32 [2048], P('tp'), may hold values from 0.1 to 1.9
- w_in: bfloat16 [2048, 2048], P(None, 'tp'), may hold values from -0.125 to 0.125
- w_mix_out: bfloat16 [2048, 2048], P(None, 'tp'), may hold values from -0.125 to 0.125
- expert_gain: float32 [2048], replicated, may hold values from 0.1 to 1.9
- expert_gate: bfloat16 [32, 2048, 2048], P('ep', None, 'tp'), may hold values from -0.125 to 0.125
- expert_up: bfloat16 [32, 2048, 2048], P('ep', None, 'tp'), may hold values from -0.125 to 0.125
- expert_down: bfloat16 [32, 2048, 2048], P('ep', None, 'tp'), may hold values from -0.125 to 0.125
- routes: int32 [16384, 2], P('ep'), may hold values from 0 to 31, all different within a row; in each aligned block of 512 rows (0 to 511, 512 to 1023, ...) at most 48 rows name the same one
- route_weight: float32 [16384, 2], P('ep'), may hold values from 0.1 to 1
Outputs:
- mixer_output: bfloat16 [16384, 2048], P('ep', 'tp')
- expert_output: bfloat16 [16384, 2048], P('ep', 'tp')
The draws below stay inside these ranges and needn't reach their ends.
Inputs may be any that keep to these rules, and one draw needn't show every extreme that they name: `routes`: each row names 2 different experts. Among the rows of one device (aligned blocks of 512 rows) no expert is named more than 48 times, a bound that some block reaches.
All inputs are finite; a program needn't handle non-finite values.
Results may differ from the reference program's by a relative error of at most 0.0071.
Values may be sent and summed in bfloat16 or wider, within the bound.
A program may use at most 64 MiB of HBM per device.

```python
import math
import jax
import jax.numpy as jnp
import numpy as np
from jax import lax

D = 2048
PW = 2048
FE = 2048
TOP = 2
TOK_DEV = 512
TOKENS = 16384
EXPERTS = 32
CAP = 48
N_EP = 32


def steps_of(own_key, dims, pieces, smallest, top_value):
    def one(axis_at, parts):
        draws = jax.random.uniform(jax.random.fold_in(jax.random.fold_in(own_key, 6), axis_at), (parts,), jnp.float32, smallest / len(pieces), top_value / len(pieces))
        return jnp.repeat(jnp.exp(draws), dims[axis_at] // parts).reshape((-1,) + (1,) * (len(dims) - axis_at - 1))

    loudness = one(*pieces[0])
    for cut in pieces[1:]:
        loudness = loudness * one(*cut)
    return loudness


def shared_out(key, own, number, rows, amount, top, most, skew):
    sequence = jax.random.permutation(key, amount)
    crowded, common = portions_of(amount, rows * top, most, skew, True), portions_of(amount, rows * top, most, skew, False)
    places = jnp.arange(amount)

    def named(tallies, turn):
        used = int((tallies > 0).sum())
        fixed = max(1, used // 4)
        moved = fixed + (places - fixed + turn * (used - fixed)) % max(1, amount - fixed)
        return jnp.zeros((amount,), jnp.int32).at[sequence[jnp.where(places < fixed, places, moved)]].set(jnp.asarray(tallies, jnp.int32))

    tallies = jnp.where(number % 4 == 0, named(crowded, number // 4), named(common, number - number // 4 - 1))
    mixed = jax.random.permutation(jax.random.fold_in(own, 3), amount)
    donor, sink = mixed[0:amount // 2 * 2:2], mixed[1:amount // 2 * 2:2]
    room = jnp.minimum(tallies[donor] - 1, most - tallies[sink]) // 2
    room = jnp.where((donor == sequence[0]) | (sink == sequence[0]) | (tallies[sink] == 0), 0, jnp.maximum(room, 0))
    moved = jax.random.randint(jax.random.fold_in(own, 4), (amount // 2,), 0, 1 << 20) % (room + 1)
    tallies = tallies.at[donor].add(-moved).at[sink].add(moved)
    members = jnp.searchsorted(jnp.cumsum(tallies), jnp.arange(rows * top), side="right").astype(jnp.int32)
    listing = members.reshape(top, rows).T
    listing = listing[jax.random.permutation(jax.random.fold_in(own, 1), rows)]
    turn = jax.random.randint(jax.random.fold_in(own, 2), (rows, 1), 0, top)
    return jnp.take_along_axis(listing, (jnp.arange(top)[None, :] + turn) % top, axis=1)


def portions_of(count, total, reach, slope, full):
    loads = [(1 << 20) // math.isqrt(grade ** slope) + 1 for grade in range(1, count + 1)]
    largest = reach if full else min(reach, max(-(-total // count), total * loads[0] // sum(loads)))
    least = 1 if total - largest >= count - 1 else 0
    holding, rest = [largest] + [least] * (count - 1), total - largest - least * (count - 1)
    while rest > 0:
        movable = [i for i in range(1, count) if holding[i] < largest] or [i for i in range(1, count) if holding[i] < reach]
        pool, remaining = sum([loads[i] for i in movable]), rest
        for i in movable:
            extra = min(reach - holding[i], max(1, remaining * loads[i] // pool), rest)
            holding[i] = holding[i] + extra
            rest = rest - extra
    return np.array(holding)


def gaussian(stream_key, extent, deviation, most, shards=(), kind=jnp.bfloat16):
    entries = jax.random.normal(stream_key, extent, jnp.float32) * deviation
    if len(shards) > 0:
        entries = steps_of(stream_key, extent, shards, -0.22, 0.18) * entries
    return jnp.clip(entries, min=-most, max=most).astype(kind)


def setup_inputs(seed: int = 0) -> dict:
    key_list = jax.random.split(jax.random.key(seed), 13)
    mixer_rows = gaussian(key_list[0], (TOKENS, D), 1.0, 6.0, ((0, 32), (1, 16)))
    expert_rows = gaussian(key_list[1], (TOKENS, D), 1.0, 6.0, ((0, 32), (1, 16)))
    mixer_gain = jnp.clip(1.0 + 0.18 * jax.random.normal(key_list[2], (D,), jnp.float32), 0.1, 1.9)
    pool_scale = jnp.clip(1.0 + 0.18 * jax.random.normal(key_list[3], (PW,), jnp.float32), 0.1, 1.9)
    w_in = gaussian(key_list[4], (D, PW), D ** -0.5, 0.125, ((1, 16),))
    w_mix_out = gaussian(key_list[5], (PW, D), PW ** -0.5, 0.125, ((1, 16),))
    expert_gain = jnp.clip(1.0 + 0.18 * jax.random.normal(key_list[6], (D,), jnp.float32), 0.1, 1.9)
    expert_gate = gaussian(key_list[7], (EXPERTS, D, FE), D ** -0.5, 0.125, ((0, 32), (2, 16)))
    expert_up = gaussian(key_list[8], (EXPERTS, D, FE), D ** -0.5, 0.125, ((0, 32), (2, 16)))
    expert_down = gaussian(key_list[9], (EXPERTS, FE, D), FE ** -0.5, 0.125, ((0, 32), (2, 16)))
    routes_keys = jax.random.split(jax.random.fold_in(key_list[10], 1), TOKENS // TOK_DEV)
    routes_turns = jax.random.permutation(jax.random.fold_in(key_list[10], 3), TOKENS // TOK_DEV)
    routes = jax.vmap(lambda own, number: shared_out(jax.random.fold_in(key_list[10], 2), own, number, TOK_DEV, EXPERTS, TOP, CAP, 1))(routes_keys, routes_turns).reshape((TOKENS, TOP))
    route_weight = jnp.clip(jnp.exp(math.log(1.0) - 2.3025851 * jax.random.uniform(key_list[11], (TOKENS, TOP), jnp.float32) ** steps_of(key_list[11], (TOKENS, TOP), ((0, 32),), -0.2, 0.2)), 0.1, 1.0)
    return {"mixer_rows": mixer_rows, "expert_rows": expert_rows, "mixer_gain": mixer_gain, "pool_scale": pool_scale, "w_in": w_in, "w_mix_out": w_mix_out, "expert_gain": expert_gain, "expert_gate": expert_gate, "expert_up": expert_up, "expert_down": expert_down, "routes": routes, "route_weight": route_weight}


norm_eps = 1e-05
pool_windows = (2, 4, 8, 16)

def layer_norm(row_block, gain_vec):
    values = row_block.astype(jnp.float32)
    center = values - lax.optimization_barrier(jnp.mean(values, axis=-1, keepdims=True))
    spread = lax.optimization_barrier(jnp.mean(center * center, axis=-1, keepdims=True))
    return (center * lax.rsqrt(spread + norm_eps) * gain_vec).astype(jnp.bfloat16)

def reference(mixer_rows, expert_rows, mixer_gain, pool_scale, w_in, w_mix_out, expert_gain, expert_gate, expert_up, expert_down, routes, route_weight):
    normed_mix = layer_norm(mixer_rows, mixer_gain)
    inner_proj = jnp.dot(normed_mix, w_in, preferred_element_type=jnp.float32).astype(jnp.bfloat16)
    values = inner_proj.astype(jnp.float32)
    seq_len = values.shape[0]
    prefix = jnp.concatenate([jnp.zeros((1, PW), jnp.float32), jnp.cumsum(values, axis=0)], axis=0)
    position = jnp.arange(seq_len, dtype=jnp.int32)
    group_width = PW // 4
    window_means = []
    for group_id, window in enumerate(pool_windows):
        lower_end = jnp.clip(position - window // 2, 0, seq_len)
        upper_end = jnp.clip(position - window // 2 + window, 0, seq_len)
        counts = (upper_end - lower_end).astype(jnp.float32)[:, None]
        columns = prefix[:, group_id * group_width:(group_id + 1) * group_width]
        window_means.append((columns[upper_end] - columns[lower_end]) / counts)
    pooled = ((jnp.concatenate(window_means, axis=1) - values) * pool_scale).astype(jnp.bfloat16)
    mixer_output = jnp.dot(pooled, w_mix_out, preferred_element_type=jnp.float32).astype(jnp.bfloat16)
    normed_expert = layer_norm(expert_rows, expert_gain)
    flat_route = routes.reshape(-1).astype(jnp.int32)
    onehot = (flat_route[:, None] == jnp.arange(EXPERTS, dtype=jnp.int32)[None, :]).astype(jnp.int32)
    running = jnp.cumsum(onehot.reshape(N_EP, TOK_DEV * TOP, EXPERTS), axis=1).reshape(-1, EXPERTS)
    ranking = lax.optimization_barrier(jnp.sum(onehot * (running - 1), axis=1))
    source_dev = jnp.arange(TOKENS * TOP, dtype=jnp.int32) // (TOK_DEV * TOP)
    slot_index = (flat_route * N_EP + source_dev) * CAP + ranking
    token_index = jnp.arange(TOKENS * TOP, dtype=jnp.int32) // TOP
    slot_table = jnp.zeros((EXPERTS * N_EP * CAP, D), jnp.bfloat16).at[slot_index].set(normed_expert[token_index])

    def run_expert(packed):
        slot_rows, gate_weight, up_weight, down_weight = packed
        gate_val = jnp.dot(slot_rows, gate_weight, preferred_element_type=jnp.float32)
        up_val = jnp.dot(slot_rows, up_weight, preferred_element_type=jnp.float32)
        hidden = (jax.nn.silu(gate_val) * up_val).astype(jnp.bfloat16)
        return jnp.dot(hidden, down_weight, preferred_element_type=jnp.float32).astype(jnp.bfloat16)
    results = lax.map(run_expert, (slot_table.reshape(EXPERTS, N_EP * CAP, D), expert_gate, expert_up, expert_down))
    picked = results.reshape(-1, D)[slot_index].astype(jnp.float32).reshape(TOKENS, TOP, D)
    expert_output = lax.optimization_barrier(jnp.sum(picked * route_weight[:, :, None], axis=1)).astype(jnp.bfloat16)
    return (mixer_output, expert_output)
```

```python
import jax
import jax.numpy as jnp
from jax import lax
from jax.experimental import pallas as pl
from jax.experimental.pallas import tpu as pltpu
from jax.sharding import PartitionSpec as P

MESH = pl.DeviceIdType.MESH
EPS = 1e-05
UNIT = 128
CAP = 48
SIDE = 4
M0, S0, P0, H0, UNITS = 0, 8, 20, 24, 36
LAG = 2
BF, F32 = jnp.bfloat16, jnp.float32


def kernel(
    mixer_ref,
    expert_ref,
    mgain_ref,
    scale_ref,
    egain_ref,
    routes_ref,
    routes_t_ref,
    rw_ref,
    w_in_hbm,
    w_mix_hbm,
    gate_hbm,
    up_hbm,
    down_hbm,
    mixer_out,
    expert_out,
    ring,
    w_in,
    w_mix,
    w_gu,
    w_down,
    outgoing,
    back,
    returned,
    normed,
    inner,
    halo,
    slot_of,
    picked,
    w_sem,
    send_sem,
    ring_sem,
    disp_send,
    disp_sem,
    back_send,
    back_sem,
    halo_send,
    halo_sem,
):
    ep, tp = lax.axis_index("ep"), lax.axis_index("tp")
    n_ep = lax.axis_size("ep")
    n_z = n_ep // 2
    rows = mixer_ref.shape[0]
    slots = n_ep * CAP
    z, core = ep // 2, ep % 2
    y, x = tp // SIDE, tp % SIDE
    yp, ym, xp, xm = (y + 1) % SIDE, (y + 3) % SIDE, (x + 1) % SIDE, (x + 3) % SIDE
    to_yp, to_ym = {"tp": yp * SIDE + x}, {"tp": ym * SIDE + x}
    to_xp, to_xm = {"tp": y * SIDE + xp}, {"tp": y * SIDE + xm}

    weights = [
        pltpu.make_async_copy(w_in_hbm, w_in, w_sem.at[0]),
        pltpu.make_async_copy(gate_hbm, w_gu.at[:, 0:128], w_sem.at[1]),
        pltpu.make_async_copy(up_hbm, w_gu.at[:, 128:256], w_sem.at[2]),
        pltpu.make_async_copy(w_mix_hbm, w_mix, w_sem.at[3]),
        pltpu.make_async_copy(down_hbm, w_down, w_sem.at[4]),
    ]
    for copy in weights:
        copy.start()

    barrier = pltpu.get_barrier_semaphore()

    def greet(j, carry):
        pl.semaphore_signal(
            barrier, inc=1, device_id={"ep": (ep + j) % n_ep}, device_id_type=MESH
        )
        return carry

    for peer in (to_yp, to_ym, to_xp, to_xm):
        pl.semaphore_signal(barrier, inc=1, device_id=peer, device_id_type=MESH)
    lax.fori_loop(1, n_ep, greet, 0)

    ring[y, x, 0:rows, :] = mixer_ref[...]

    half = n_z // 2

    def step_of(q):
        j = q // 2
        return jnp.where(j % 2 == 1, half - (j + 1) // 2, j // 2 - half)

    q_col = lax.broadcasted_iota(jnp.int32, (n_ep, 1), 0)
    q_row = lax.broadcasted_iota(jnp.int32, (1, n_ep), 1)

    def expert_at(q):
        other = (core + q % 2) % 2
        return (z + step_of(q) + n_z) % n_z * 2 + other

    e_col = expert_at(q_col)
    named = (routes_t_ref[0:1, :] == e_col) | (routes_t_ref[1:2, :] == e_col)
    r_iota = lax.broadcasted_iota(jnp.int32, (rows, rows), 0)
    c_iota = lax.broadcasted_iota(jnp.int32, (rows, rows), 1)
    before = jnp.where(r_iota < c_iota, 1.0, 0.0).astype(BF)
    rank = jnp.dot(
        jnp.where(named, 1.0, 0.0).astype(BF), before, preferred_element_type=F32
    )
    rank = jnp.where(named, rank, -1.0)
    place = lax.broadcasted_iota(jnp.int32, (CAP, rows), 0).astype(F32)
    for g in range(n_ep // 8):
        hot = jnp.concatenate(
            [
                jnp.where(rank[q : q + 1, :] == place, 1.0, 0.0).astype(BF)
                for q in range(8 * g, 8 * g + 8)
            ],
            axis=0,
        )
        outgoing[8 * CAP * g : 8 * CAP * (g + 1), :] = jnp.dot(
            hot, expert_ref[...], preferred_element_type=F32
        ).astype(BF)
    own = (n_ep - 2) * CAP
    ring[y, x, S0 * UNIT + own : S0 * UNIT + own + CAP, :] = outgoing[own : own + CAP, :]

    pl.semaphore_wait(barrier, n_ep - 1 + 4)

    def remote(src, dst, send, recv, device):
        pltpu.make_async_remote_copy(
            src_ref=src,
            dst_ref=dst,
            send_sem=send,
            recv_sem=recv,
            device_id=device,
            device_id_type=MESH,
        ).start()

    def await_bytes(ref, sem):
        pltpu.make_async_copy(ref, ref, sem).wait()

    def ring_copy(ref, sem, device):
        remote(ref, ref, send_sem, sem, device)

    def first_a(u):
        r = u * UNIT
        lo, hi = pl.ds(r, 64), pl.ds(r + 64, 64)
        ring_copy(ring.at[y, x, lo], ring_sem.at[u, 0, 0], to_xp)
        ring_copy(ring.at[y, x, hi], ring_sem.at[u, 1, 0], to_yp)
        ring_copy(ring.at[y, x, lo], ring_sem.at[u, 0, 0], to_xm)
        ring_copy(ring.at[y, x, hi], ring_sem.at[u, 1, 0], to_ym)

    def second_a(u):
        r = u * UNIT
        await_bytes(ring.at[y, x, pl.ds(r, 128)], ring_sem.at[u, 0, 0])
        await_bytes(ring.at[y, x, pl.ds(r, 128)], ring_sem.at[u, 1, 0])
        ring_copy(ring.at[y, xm, pl.ds(r, 32)], ring_sem.at[u, 0, 1], to_xp)
        ring_copy(ring.at[ym, x, pl.ds(r + 64, 32)], ring_sem.at[u, 1, 1], to_yp)
        ring_copy(ring.at[y, xp, pl.ds(r + 32, 32)], ring_sem.at[u, 0, 1], to_xm)
        ring_copy(ring.at[yp, x, pl.ds(r + 96, 32)], ring_sem.at[u, 1, 1], to_ym)

    def first_b(u):
        r = u * UNIT
        lo, hi = pl.ds(r, 64), pl.ds(r + 64, 64)
        await_bytes(ring.at[y, x, lo], ring_sem.at[u, 0, 1])
        await_bytes(ring.at[y, x, lo], ring_sem.at[u, 1, 1])
        ring_copy(ring.at[y, :, lo], ring_sem.at[u, 0, 2], to_yp)
        ring_copy(ring.at[:, x, hi], ring_sem.at[u, 1, 2], to_xp)
        ring_copy(ring.at[y, :, lo], ring_sem.at[u, 0, 2], to_ym)
        ring_copy(ring.at[:, x, hi], ring_sem.at[u, 1, 2], to_xm)

    def second_b(u):
        r = u * UNIT
        await_bytes(ring.at[y, :, pl.ds(r, 128)], ring_sem.at[u, 0, 2])
        await_bytes(ring.at[y, :, pl.ds(r, 128)], ring_sem.at[u, 1, 2])
        ring_copy(ring.at[ym, :, pl.ds(r, 32)], ring_sem.at[u, 0, 3], to_yp)
        ring_copy(ring.at[:, xm, pl.ds(r + 64, 32)], ring_sem.at[u, 1, 3], to_xp)
        ring_copy(ring.at[yp, :, pl.ds(r + 32, 32)], ring_sem.at[u, 0, 3], to_ym)
        ring_copy(ring.at[:, xp, pl.ds(r + 96, 32)], ring_sem.at[u, 1, 3], to_xm)

    def finished(u):
        r = u * UNIT
        await_bytes(ring.at[y, :, pl.ds(r, 64)], ring_sem.at[u, 0, 3])
        await_bytes(ring.at[y, :, pl.ds(r, 64)], ring_sem.at[u, 1, 3])

    def peer_at(q, sign):
        dz = half - (q // 2 + 1) // 2 if (q // 2) % 2 == 1 else q // 2 // 2 - half
        other = (core + q % 2) % 2
        return {"ep": (z + sign * dz + n_z) % n_z * 2 + other}

    for q in range(n_ep):
        if q != n_ep - 2:
            remote(
                outgoing.at[q * CAP : (q + 1) * CAP],
                ring.at[y, x, S0 * UNIT + q * CAP : S0 * UNIT + (q + 1) * CAP],
                disp_send,
                disp_sem.at[q // 8],
                peer_at(q, 1),
            )

    e_row = expert_at(q_row)
    hits = [routes_ref[:, k : k + 1] == e_row for k in range(2)]
    after = jnp.where(c_iota < r_iota, 1.0, 0.0).astype(BF)
    rank_c = jnp.dot(
        after, jnp.where(hits[0] | hits[1], 1.0, 0.0).astype(BF), preferred_element_type=F32
    )
    base = q_row.astype(F32) * float(CAP)
    for k in range(2):
        at = jnp.sum(jnp.where(hits[k], rank_c + base, 0.0), axis=1, keepdims=True)
        slot_of[k * rows : (k + 1) * rows, :] = jnp.broadcast_to(at, (rows, 128))
    picked[...] = jnp.zeros_like(picked)

    def layer_norm(u, gain_ref):
        def block(b, carry):
            r = pl.ds(u * UNIT + b * 32, 32)

            def piece(p):
                return ring[p // SIDE, p % SIDE, r, :].astype(F32)

            n = SIDE * SIDE
            total = piece(0)
            for p in range(1, n):
                total = total + piece(p)
            mean = jnp.sum(total, axis=1, keepdims=True) * (1.0 / (n * 128))
            square = None
            for p in range(n):
                d = piece(p) - mean
                square = d * d if square is None else square + d * d
            var = jnp.sum(square, axis=1, keepdims=True) * (1.0 / (n * 128))
            inv = lax.rsqrt(var + EPS)
            for p in range(n):
                normed[pl.ds(b * 32, 32), p * 128 : (p + 1) * 128] = (
                    (piece(p) - mean) * inv * gain_ref[p : p + 1, :]
                ).astype(BF)
            return carry

        lax.fori_loop(0, UNIT // 32, block, 0)

    def wide(u):
        r = pl.ds(u * UNIT, UNIT)
        return jnp.concatenate(
            [ring[p // SIDE, p % SIDE, r, :] for p in range(SIDE * SIDE)], axis=1
        )

    def mixer_unit(u):
        layer_norm(u, mgain_ref)
        inner[pl.ds((u - M0) * UNIT, UNIT), :] = jnp.dot(
            normed[...], w_in[...], preferred_element_type=F32
        ).astype(BF)

    def slot_unit(u):
        layer_norm(u, egain_ref)
        both = jnp.dot(normed[...], w_gu[...], preferred_element_type=F32)
        gate, up = both[:, 0:128], both[:, 128:256]
        hidden = gate / (1.0 + jnp.exp(-gate)) * up
        ring[y, x, pl.ds((u - S0 + H0) * UNIT, UNIT), :] = hidden.astype(BF)

    def pooled_unit(u):
        mixer_out[pl.ds((u - P0) * UNIT, UNIT), :] = jnp.dot(
            wide(u), w_mix[...], preferred_element_type=F32
        ).astype(BF)

    def hidden_unit(u):
        back[pl.ds((u - H0) * UNIT, UNIT), :] = jnp.dot(
            wide(u), w_down[...], preferred_element_type=F32
        ).astype(BF)

    def halo_out():
        remote(
            inner.at[rows - 16 : rows],
            halo.at[0:16],
            halo_send,
            halo_sem.at[0],
            {"ep": (ep + 1) % n_ep},
        )
        remote(
            inner.at[0:16],
            halo.at[16:32],
            halo_send,
            halo_sem.at[1],
            {"ep": (ep + n_ep - 1) % n_ep},
        )

    def pool():
        await_bytes(halo.at[0:16], halo_sem.at[0])
        await_bytes(halo.at[16:32], halo_sem.at[1])
        low = jnp.where(ep > 0, halo[8:16, :].astype(F32), 0.0)
        high = jnp.where(ep < n_ep - 1, halo[16:24, :].astype(F32), 0.0)
        values = inner[...].astype(F32)
        ext = jnp.concatenate([low, values, high], axis=0)
        two = ext[0 : rows + 15, :] + ext[1 : rows + 16, :]
        four = two[0 : rows + 13, :] + two[2 : rows + 15, :]
        eight = four[0 : rows + 9, :] + four[4 : rows + 13, :]
        sixteen = eight[0 : rows + 1, :] + eight[8 : rows + 9, :]
        total = jnp.where(
            y == 0,
            two[7 : 7 + rows, :],
            jnp.where(
                y == 1,
                four[6 : 6 + rows, :],
                jnp.where(y == 2, eight[4 : 4 + rows, :], sixteen[0:rows, :]),
            ),
        )
        reach = jnp.where(y == 0, 1, jnp.where(y == 1, 2, jnp.where(y == 2, 4, 8)))
        token = ep * rows + lax.broadcasted_iota(jnp.int32, (rows, 128), 0)
        count = jnp.minimum(token + reach, n_ep * rows) - jnp.maximum(token - reach, 0)
        result = (total / count.astype(F32) - values) * scale_ref[...]
        ring[y, x, P0 * UNIT : P0 * UNIT + rows, :] = result.astype(BF)

    def send_back(g):
        for q in range(8 * g, 8 * g + 8):
            part = slice(q * CAP, (q + 1) * CAP)
            if q == n_ep - 2:
                returned[part, :] = back[part, :]
            else:
                remote(
                    back.at[part], returned.at[part], back_send, back_sem.at[g], peer_at(q, -1)
                )

    group = 8 * CAP
    lane = lax.broadcasted_iota(jnp.int32, (2 * rows, 128), 1).astype(F32)

    def combine(g):
        count = group if 8 * g + 8 < n_ep else group - CAP
        await_bytes(returned.at[0:count], back_sem.at[g])
        where = slot_of[...]
        hot = jnp.concatenate(
            [
                jnp.where(where == lane + float(g * group + c * 128), 1.0, 0.0).astype(BF)
                for c in range(group // 128)
            ],
            axis=1,
        )
        picked[...] += jnp.dot(
            hot, returned[g * group : (g + 1) * group, :], preferred_element_type=F32
        )

    n_groups = n_ep // 8

    def sends(u):
        return ((u >= M0) & (u < M0 + rows // UNIT)) | ((u >= S0) & (u < UNITS))

    def step(i, carry):
        for lag, stage in ((3 * LAG, second_b), (2 * LAG, first_b), (LAG, second_a)):
            u = i - lag

            @pl.when(sends(u))
            def _():
                stage(u)

        for g in range(n_groups):

            @pl.when(i == S0 + 3 * g)
            def _():
                count = group if g + 1 < n_groups else group - CAP
                await_bytes(ring.at[y, x, 0:count], disp_sem.at[g])

        @pl.when(sends(i))
        def _():
            first_a(i)

        u = i - 4 * LAG

        @pl.when(sends(u))
        def _():
            finished(u)

        @pl.when(u == M0)
        def _():
            for copy in weights:
                copy.wait()

        @pl.when((u >= M0) & (u < M0 + rows // UNIT))
        def _():
            mixer_unit(u)

        @pl.when(u == M0 + rows // UNIT - 1)
        def _():
            halo_out()

        @pl.when(u == M0 + rows // UNIT + 2)
        def _():
            pool()

        @pl.when((u >= S0) & (u < P0))
        def _():
            slot_unit(u)

        @pl.when((u >= P0) & (u < H0))
        def _():
            pooled_unit(u)

        @pl.when(u >= H0)
        def _():
            hidden_unit(u)

        for g in range(n_groups):

            @pl.when(u == H0 + 3 * g + 2)
            def _():
                if g > 0:
                    combine(g - 1)
                send_back(g)

        return carry

    lax.fori_loop(0, UNITS + 4 * LAG, step, 0)
    combine(n_groups - 1)
    expert_out[...] = (
        picked[0:rows, :] * rw_ref[:, 0:1] + picked[rows : 2 * rows, :] * rw_ref[:, 1:2]
    ).astype(BF)
    sent = (SIDE * SIDE - 1) * (2 * rows + 2 * slots) // (SIDE * SIDE)
    await_bytes(ring.at[:, :, 0:sent], send_sem)
    await_bytes(outgoing.at[0 : slots - CAP], disp_send)
    await_bytes(back.at[0 : slots - CAP], back_send)
    await_bytes(inner.at[0:32], halo_send)


def on_device(
    mixer_rows,
    expert_rows,
    mixer_gain,
    pool_scale,
    w_in,
    w_mix_out,
    expert_gain,
    expert_gate,
    expert_up,
    expert_down,
    routes,
    route_weight,
):
    rows, feats = mixer_rows.shape
    n_ep = lax.axis_size("ep")
    depth = w_in.shape[0]
    vmem = pl.BlockSpec(memory_space=pltpu.VMEM)
    hbm = pl.BlockSpec(memory_space=pl.ANY)
    slots = n_ep * CAP
    return pl.pallas_call(
        kernel,
        name="mixer_and_experts",
        out_shape=(
            jax.ShapeDtypeStruct((rows, feats), BF),
            jax.ShapeDtypeStruct((rows, feats), BF),
        ),
        in_specs=[vmem] * 8 + [hbm] * 5,
        out_specs=(vmem, vmem),
        scratch_shapes=[
            pltpu.VMEM((SIDE, SIDE, UNITS * UNIT, feats), BF),
            pltpu.VMEM((depth, 128), BF),
            pltpu.VMEM((depth, 128), BF),
            pltpu.VMEM((depth, 256), BF),
            pltpu.VMEM((depth, 128), BF),
            pltpu.VMEM((slots, feats), BF),
            pltpu.VMEM((slots, feats), BF),
            pltpu.VMEM((slots, feats), BF),
            pltpu.VMEM((UNIT, depth), BF),
            pltpu.VMEM((rows, feats), BF),
            pltpu.VMEM((32, feats), BF),
            pltpu.VMEM((2 * rows, 128), F32),
            pltpu.VMEM((2 * rows, feats), F32),
            pltpu.SemaphoreType.DMA((5,)),
            pltpu.SemaphoreType.DMA,
            pltpu.SemaphoreType.DMA((UNITS, 2, 4)),
            pltpu.SemaphoreType.DMA,
            pltpu.SemaphoreType.DMA((n_ep // 8,)),
            pltpu.SemaphoreType.DMA,
            pltpu.SemaphoreType.DMA((n_ep // 8,)),
            pltpu.SemaphoreType.DMA,
            pltpu.SemaphoreType.DMA((2,)),
        ],
        compiler_params=pltpu.CompilerParams(
            collective_id=0, has_side_effects=True, vmem_limit_bytes=60 * 1024 * 1024
        ),
    )(
        mixer_rows,
        expert_rows,
        mixer_gain.reshape(-1, 128),
        pool_scale.reshape(1, -1),
        expert_gain.reshape(-1, 128),
        routes,
        routes.T,
        route_weight,
        w_in,
        w_mix_out,
        expert_gate[0],
        expert_up[0],
        expert_down[0],
    )


def solution(mesh):
    return jax.shard_map(
        on_device,
        mesh=mesh,
        in_specs=(
            P("ep", "tp"),
            P("ep", "tp"),
            P(),
            P("tp"),
            P(None, "tp"),
            P(None, "tp"),
            P(),
            P("ep", None, "tp"),
            P("ep", None, "tp"),
            P("ep", None, "tp"),
            P("ep", None),
            P("ep", None),
        ),
        out_specs=(P("ep", "tp"), P("ep", "tp")),
        check_vma=False,
    )
```

```python
import jax
import jax.numpy as jnp
from jax import lax
from jax.experimental import pallas as pl
from jax.experimental.pallas import tpu as pltpu
from jax.sharding import PartitionSpec as P

MESH = pl.DeviceIdType.MESH
EPS = 1e-05
UNIT = 128
CAP = 48
SIDE = 4
M0, S0, H0, P0, UNITS = 0, 4, 16, 28, 32
LAG = 2
BF, F32 = jnp.bfloat16, jnp.float32


def kernel(
    mixer_ref,
    expert_ref,
    mgain_ref,
    scale_ref,
    egain_ref,
    routes_t_ref,
    rw_t_ref,
    w_in_hbm,
    w_mix_hbm,
    gate_hbm,
    up_hbm,
    down_hbm,
    mixer_out,
    expert_out,
    ring,
    w_in,
    w_mix,
    w_gu,
    w_down,
    outgoing,
    back,
    returned,
    normed,
    inner,
    halo,
    slot_of,
    weight_of,
    ranks,
    picked,
    w_sem,
    send_sem,
    ring_sem,
    disp_send,
    disp_sem,
    back_send,
    back_sem,
    halo_send,
    halo_sem,
):
    ep, tp = lax.axis_index("ep"), lax.axis_index("tp")
    n_ep = lax.axis_size("ep")
    n_z = n_ep // 2
    rows = mixer_ref.shape[0]
    slots = n_ep * CAP
    z, core = ep // 2, ep % 2
    y, x = tp // SIDE, tp % SIDE
    yp, ym, xp, xm = (y + 1) % SIDE, (y + 3) % SIDE, (x + 1) % SIDE, (x + 3) % SIDE
    to_yp, to_ym = {"tp": yp * SIDE + x}, {"tp": ym * SIDE + x}
    to_xp, to_xm = {"tp": y * SIDE + xp}, {"tp": y * SIDE + xm}

    weights = [
        pltpu.make_async_copy(w_in_hbm, w_in, w_sem.at[0]),
        pltpu.make_async_copy(gate_hbm, w_gu.at[:, 0:128], w_sem.at[1]),
        pltpu.make_async_copy(up_hbm, w_gu.at[:, 128:256], w_sem.at[2]),
        pltpu.make_async_copy(w_mix_hbm, w_mix, w_sem.at[3]),
        pltpu.make_async_copy(down_hbm, w_down, w_sem.at[4]),
    ]
    for copy in weights:
        copy.start()

    barrier = pltpu.get_barrier_semaphore()

    def greet(j, carry):
        pl.semaphore_signal(
            barrier, inc=1, device_id={"ep": (ep + j) % n_ep}, device_id_type=MESH
        )
        return carry

    for peer in (to_yp, to_ym, to_xp, to_xm):
        pl.semaphore_signal(barrier, inc=1, device_id=peer, device_id_type=MESH)
    lax.fori_loop(1, n_ep, greet, 0)

    ring[y, x, 0:rows, :] = mixer_ref[...]

    def step_of(q):
        j = q // 2
        return jnp.where(j % 2 == 1, (j + 1) // 2, 0 - j // 2)

    q_col = lax.broadcasted_iota(jnp.int32, (n_ep, 1), 0)

    def expert_at(q):
        other = (core + q % 2) % 2
        return (z + step_of(q) + n_z) % n_z * 2 + other

    e_col = expert_at(q_col)
    named = (routes_t_ref[0:1, :] == e_col) | (routes_t_ref[1:2, :] == e_col)
    r_iota = lax.broadcasted_iota(jnp.int32, (rows, rows), 0)
    c_iota = lax.broadcasted_iota(jnp.int32, (rows, rows), 1)
    before = jnp.where(r_iota < c_iota, 1.0, 0.0).astype(BF)
    rank = jnp.dot(
        jnp.where(named, 1.0, 0.0).astype(BF), before, preferred_element_type=F32
    )
    rank = jnp.where(named, rank, -1.0)
    ranks[...] = rank
    place = lax.broadcasted_iota(jnp.int32, (CAP, rows), 0).astype(F32)
    for g in range(n_ep // 8):
        hot = jnp.concatenate(
            [
                jnp.where(rank[q : q + 1, :] == place, 1.0, 0.0).astype(BF)
                for q in range(8 * g, 8 * g + 8)
            ],
            axis=0,
        )
        outgoing[8 * CAP * g : 8 * CAP * (g + 1), :] = jnp.dot(
            hot, expert_ref[...], preferred_element_type=F32
        ).astype(BF)
    ring[y, x, S0 * UNIT : S0 * UNIT + CAP, :] = outgoing[0:CAP, :]

    pl.semaphore_wait(barrier, n_ep - 1 + 4)

    def remote(src, dst, send, recv, device):
        pltpu.make_async_remote_copy(
            src_ref=src,
            dst_ref=dst,
            send_sem=send,
            recv_sem=recv,
            device_id=device,
            device_id_type=MESH,
        ).start()

    def await_bytes(ref, sem):
        pltpu.make_async_copy(ref, ref, sem).wait()

    def ring_copy(ref, sem, device):
        remote(ref, ref, send_sem, sem, device)

    def first_a(u):
        r = u * UNIT
        lo, hi = pl.ds(r, 64), pl.ds(r + 64, 64)
        ring_copy(ring.at[y, x, lo], ring_sem.at[u, 0, 0], to_xp)
        ring_copy(ring.at[y, x, hi], ring_sem.at[u, 1, 0], to_yp)
        ring_copy(ring.at[y, x, lo], ring_sem.at[u, 0, 0], to_xm)
        ring_copy(ring.at[y, x, hi], ring_sem.at[u, 1, 0], to_ym)

    def second_a(u):
        r = u * UNIT
        await_bytes(ring.at[y, x, pl.ds(r, 128)], ring_sem.at[u, 0, 0])
        await_bytes(ring.at[y, x, pl.ds(r, 128)], ring_sem.at[u, 1, 0])
        ring_copy(ring.at[y, xm, pl.ds(r, 32)], ring_sem.at[u, 0, 1], to_xp)
        ring_copy(ring.at[ym, x, pl.ds(r + 64, 32)], ring_sem.at[u, 1, 1], to_yp)
        ring_copy(ring.at[y, xp, pl.ds(r + 32, 32)], ring_sem.at[u, 0, 1], to_xm)
        ring_copy(ring.at[yp, x, pl.ds(r + 96, 32)], ring_sem.at[u, 1, 1], to_ym)

    def first_b(u):
        r = u * UNIT
        lo, hi = pl.ds(r, 64), pl.ds(r + 64, 64)
        await_bytes(ring.at[y, x, lo], ring_sem.at[u, 0, 1])
        await_bytes(ring.at[y, x, lo], ring_sem.at[u, 1, 1])
        ring_copy(ring.at[y, :, lo], ring_sem.at[u, 0, 2], to_yp)
        ring_copy(ring.at[:, x, hi], ring_sem.at[u, 1, 2], to_xp)
        ring_copy(ring.at[y, :, lo], ring_sem.at[u, 0, 2], to_ym)
        ring_copy(ring.at[:, x, hi], ring_sem.at[u, 1, 2], to_xm)

    def second_b(u):
        r = u * UNIT
        await_bytes(ring.at[y, :, pl.ds(r, 128)], ring_sem.at[u, 0, 2])
        await_bytes(ring.at[y, :, pl.ds(r, 128)], ring_sem.at[u, 1, 2])
        ring_copy(ring.at[ym, :, pl.ds(r, 32)], ring_sem.at[u, 0, 3], to_yp)
        ring_copy(ring.at[:, xm, pl.ds(r + 64, 32)], ring_sem.at[u, 1, 3], to_xp)
        ring_copy(ring.at[yp, :, pl.ds(r + 32, 32)], ring_sem.at[u, 0, 3], to_ym)
        ring_copy(ring.at[:, xp, pl.ds(r + 96, 32)], ring_sem.at[u, 1, 3], to_xm)

    def finished(u):
        r = u * UNIT
        await_bytes(ring.at[y, :, pl.ds(r, 64)], ring_sem.at[u, 0, 3])
        await_bytes(ring.at[y, :, pl.ds(r, 64)], ring_sem.at[u, 1, 3])

    def peer_at(q, sign):
        dz = (q // 2 + 1) // 2 if (q // 2) % 2 == 1 else -(q // 2 // 2)
        other = (core + q % 2) % 2
        return {"ep": (z + sign * dz + n_z) % n_z * 2 + other}

    for u in range(M0, M0 + rows // UNIT):
        first_a(u)
    for q in range(1, n_ep):
        remote(
            outgoing.at[q * CAP : (q + 1) * CAP],
            ring.at[y, x, S0 * UNIT + q * CAP : S0 * UNIT + (q + 1) * CAP],
            disp_send,
            disp_sem.at[q // 8],
            peer_at(q, 1),
        )

    def place_results():
        e_at = expert_at(q_col)
        base = q_col.astype(F32) * float(CAP)
        for k in range(2):
            mine = routes_t_ref[k : k + 1, :] == e_at
            at = jnp.sum(jnp.where(mine, ranks[...] + base, 0.0), axis=0, keepdims=True)
            part = slice(k * rows, (k + 1) * rows)
            slot_of[part, :] = jnp.broadcast_to(at, (128, rows)).T
            weight_of[part, :] = jnp.broadcast_to(rw_t_ref[k : k + 1, :], (128, rows)).T

    picked[...] = jnp.zeros_like(picked)

    def layer_norm(u, gain_ref):
        def block(b, carry):
            r = pl.ds(u * UNIT + b * 32, 32)

            def piece(p):
                return ring[p // SIDE, p % SIDE, r, :].astype(F32)

            n = SIDE * SIDE
            total = piece(0)
            for p in range(1, n):
                total = total + piece(p)
            mean = jnp.sum(total, axis=1, keepdims=True) * (1.0 / (n * 128))
            square = None
            for p in range(n):
                d = piece(p) - mean
                square = d * d if square is None else square + d * d
            var = jnp.sum(square, axis=1, keepdims=True) * (1.0 / (n * 128))
            inv = lax.rsqrt(var + EPS)
            for p in range(n):
                normed[pl.ds(b * 32, 32), p * 128 : (p + 1) * 128] = (
                    (piece(p) - mean) * inv * gain_ref[p : p + 1, :]
                ).astype(BF)
            return carry

        lax.fori_loop(0, UNIT // 32, block, 0)

    def wide(u):
        r = pl.ds(u * UNIT, UNIT)
        return jnp.concatenate(
            [ring[p // SIDE, p % SIDE, r, :] for p in range(SIDE * SIDE)], axis=1
        )

    def mixer_unit(u):
        layer_norm(u, mgain_ref)
        inner[pl.ds((u - M0) * UNIT, UNIT), :] = jnp.dot(
            normed[...], w_in[...], preferred_element_type=F32
        ).astype(BF)

    def slot_unit(u):
        layer_norm(u, egain_ref)
        both = jnp.dot(normed[...], w_gu[...], preferred_element_type=F32)
        gate, up = both[:, 0:128], both[:, 128:256]
        hidden = gate / (1.0 + jnp.exp(-gate)) * up
        ring[y, x, pl.ds((u - S0 + H0) * UNIT, UNIT), :] = hidden.astype(BF)

    def pooled_unit(u):
        mixer_out[pl.ds((u - P0) * UNIT, UNIT), :] = jnp.dot(
            wide(u), w_mix[...], preferred_element_type=F32
        ).astype(BF)

    def hidden_unit(u):
        back[pl.ds((u - H0) * UNIT, UNIT), :] = jnp.dot(
            wide(u), w_down[...], preferred_element_type=F32
        ).astype(BF)

    def halo_out():
        remote(
            inner.at[rows - 16 : rows],
            halo.at[0:16],
            halo_send,
            halo_sem.at[0],
            {"ep": (ep + 1) % n_ep},
        )
        remote(
            inner.at[0:16],
            halo.at[16:32],
            halo_send,
            halo_sem.at[1],
            {"ep": (ep + n_ep - 1) % n_ep},
        )

    def pool():
        await_bytes(halo.at[0:16], halo_sem.at[0])
        await_bytes(halo.at[16:32], halo_sem.at[1])
        low = jnp.where(ep > 0, halo[8:16, :].astype(F32), 0.0)
        high = jnp.where(ep < n_ep - 1, halo[16:24, :].astype(F32), 0.0)
        values = inner[...].astype(F32)
        ext = jnp.concatenate([low, values, high], axis=0)
        two = ext[0 : rows + 15, :] + ext[1 : rows + 16, :]
        four = two[0 : rows + 13, :] + two[2 : rows + 15, :]
        eight = four[0 : rows + 9, :] + four[4 : rows + 13, :]
        sixteen = eight[0 : rows + 1, :] + eight[8 : rows + 9, :]
        total = jnp.where(
            y == 0,
            two[7 : 7 + rows, :],
            jnp.where(
                y == 1,
                four[6 : 6 + rows, :],
                jnp.where(y == 2, eight[4 : 4 + rows, :], sixteen[0:rows, :]),
            ),
        )
        reach = jnp.where(y == 0, 1, jnp.where(y == 1, 2, jnp.where(y == 2, 4, 8)))
        token = ep * rows + lax.broadcasted_iota(jnp.int32, (rows, 128), 0)
        count = jnp.minimum(token + reach, n_ep * rows) - jnp.maximum(token - reach, 0)
        result = (total / count.astype(F32) - values) * scale_ref[...]
        ring[y, x, P0 * UNIT : P0 * UNIT + rows, :] = result.astype(BF)

    def send_back(g):
        for q in range(8 * g, 8 * g + 8):
            part = slice(q * CAP, (q + 1) * CAP)
            if q == 0:
                returned[part, :] = back[part, :]
            else:
                remote(
                    back.at[part], returned.at[part], back_send, back_sem.at[g], peer_at(q, -1)
                )

    group = 8 * CAP
    lane = lax.broadcasted_iota(jnp.int32, (2 * rows, 128), 1).astype(F32)

    def combine(g):
        count = group if g > 0 else group - CAP
        await_bytes(returned.at[0:count], back_sem.at[g])
        where = slot_of[...]
        hot = jnp.concatenate(
            [
                jnp.where(where == lane + float(g * group + c * 128), 1.0, 0.0).astype(BF)
                for c in range(group // 128)
            ],
            axis=1,
        )
        picked[...] += jnp.dot(
            hot, returned[g * group : (g + 1) * group, :], preferred_element_type=F32
        )

    n_groups = n_ep // 8

    def sends(u):
        return ((u >= M0) & (u < M0 + rows // UNIT)) | ((u >= S0) & (u < UNITS))

    def step(i, carry):
        for lag, stage in ((3 * LAG, second_b), (2 * LAG, first_b), (LAG, second_a)):
            u = i - lag

            @pl.when(sends(u))
            def _():
                stage(u)

        for g in range(n_groups):

            @pl.when(i == S0 + 3 * g)
            def _():
                count = group if g > 0 else group - CAP
                await_bytes(ring.at[y, x, 0:count], disp_sem.at[g])

        @pl.when((i >= S0) & (i < UNITS))
        def _():
            first_a(i)

        @pl.when(i == S0 + 4)
        def _():
            place_results()

        u = i - 4 * LAG

        @pl.when(u == UNITS - 1)
        def _():
            combine(n_groups - 1)
            expert_out[...] = (
                picked[0:rows, :] * weight_of[0:rows, :]
                + picked[rows : 2 * rows, :] * weight_of[rows : 2 * rows, :]
            ).astype(BF)

        @pl.when(sends(u))
        def _():
            finished(u)

        @pl.when(u == M0)
        def _():
            for copy in weights:
                copy.wait()

        @pl.when((u >= M0) & (u < M0 + rows // UNIT))
        def _():
            mixer_unit(u)

        @pl.when(u == M0 + rows // UNIT - 1)
        def _():
            halo_out()

        @pl.when(u == M0 + rows // UNIT + 2)
        def _():
            pool()

        @pl.when((u >= S0) & (u < H0))
        def _():
            slot_unit(u)

        @pl.when(u >= P0)
        def _():
            pooled_unit(u)

        @pl.when((u >= H0) & (u < P0))
        def _():
            hidden_unit(u)

        for g in range(n_groups):

            @pl.when(u == H0 + 3 * g + 2)
            def _():
                if g > 0:
                    combine(g - 1)
                send_back(g)

        return carry

    lax.fori_loop(0, UNITS + 4 * LAG, step, 0)
    sent = (SIDE * SIDE - 1) * (2 * rows + 2 * slots) // (SIDE * SIDE)
    await_bytes(ring.at[:, :, 0:sent], send_sem)
    await_bytes(outgoing.at[0 : slots - CAP], disp_send)
    await_bytes(back.at[0 : slots - CAP], back_send)
    await_bytes(inner.at[0:32], halo_send)


def on_device(
    mixer_rows,
    expert_rows,
    mixer_gain,
    pool_scale,
    w_in,
    w_mix_out,
    expert_gain,
    expert_gate,
    expert_up,
    expert_down,
    routes,
    route_weight,
):
    rows, feats = mixer_rows.shape
    n_ep = lax.axis_size("ep")
    depth = w_in.shape[0]
    vmem = pl.BlockSpec(memory_space=pltpu.VMEM)
    hbm = pl.BlockSpec(memory_space=pl.ANY)
    slots = n_ep * CAP
    return pl.pallas_call(
        kernel,
        name="mixer_and_experts",
        out_shape=(
            jax.ShapeDtypeStruct((rows, feats), BF),
            jax.ShapeDtypeStruct((rows, feats), BF),
        ),
        in_specs=[vmem] * 7 + [hbm] * 5,
        out_specs=(vmem, vmem),
        scratch_shapes=[
            pltpu.VMEM((SIDE, SIDE, UNITS * UNIT, feats), BF),
            pltpu.VMEM((depth, 128), BF),
            pltpu.VMEM((depth, 128), BF),
            pltpu.VMEM((depth, 256), BF),
            pltpu.VMEM((depth, 128), BF),
            pltpu.VMEM((slots, feats), BF),
            pltpu.VMEM((slots, feats), BF),
            pltpu.VMEM((slots, feats), BF),
            pltpu.VMEM((UNIT, depth), BF),
            pltpu.VMEM((rows, feats), BF),
            pltpu.VMEM((32, feats), BF),
            pltpu.VMEM((2 * rows, 128), F32),
            pltpu.VMEM((2 * rows, 128), F32),
            pltpu.VMEM((n_ep, rows), F32),
            pltpu.VMEM((2 * rows, feats), F32),
            pltpu.SemaphoreType.DMA((5,)),
            pltpu.SemaphoreType.DMA,
            pltpu.SemaphoreType.DMA((UNITS, 2, 4)),
            pltpu.SemaphoreType.DMA,
            pltpu.SemaphoreType.DMA((n_ep // 8,)),
            pltpu.SemaphoreType.DMA,
            pltpu.SemaphoreType.DMA((n_ep // 8,)),
            pltpu.SemaphoreType.DMA,
            pltpu.SemaphoreType.DMA((2,)),
        ],
        compiler_params=pltpu.CompilerParams(
            collective_id=0, has_side_effects=True, vmem_limit_bytes=60 * 1024 * 1024
        ),
    )(
        mixer_rows,
        expert_rows,
        mixer_gain.reshape(-1, 128),
        pool_scale.reshape(1, -1),
        expert_gain.reshape(-1, 128),
        routes.T,
        route_weight.T,
        w_in,
        w_mix_out,
        expert_gate[0],
        expert_up[0],
        expert_down[0],
    )


def solution(mesh):
    return jax.shard_map(
        on_device,
        mesh=mesh,
        in_specs=(
            P("ep", "tp"),
            P("ep", "tp"),
            P(),
            P("tp"),
            P(None, "tp"),
            P(None, "tp"),
            P(),
            P("ep", None, "tp"),
            P("ep", None, "tp"),
            P("ep", None, "tp"),
            P("ep", None),
            P("ep", None),
        ),
        out_specs=(P("ep", "tp"), P("ep", "tp")),
        check_vma=False,
    )
```

```python
import jax
import jax.numpy as jnp
from jax import lax
from jax.experimental import pallas as pl
from jax.experimental.pallas import tpu as pltpu
from jax.sharding import PartitionSpec as P

MESH = pl.DeviceIdType.MESH
EPS = 1e-05
UNIT = 128
SLOT_UNITS, TURN = 12, 3
CAP = 48
SIDE = 4
M0, S0, H0, P0, UNITS = 0, 4, 16, 28, 32
A2, B1, B2, DONE = 2, 4, 6, 8
BF, F32 = jnp.bfloat16, jnp.float32


def kernel(
    mixer_hbm,
    expert_hbm,
    mgain_hbm,
    scale_hbm,
    egain_hbm,
    routes_t_hbm,
    rw_t_hbm,
    w_in_hbm,
    w_mix_hbm,
    gate_hbm,
    up_hbm,
    down_hbm,
    out,
    ring,
    w_in,
    w_mix,
    w_gu,
    w_down,
    outgoing,
    back,
    returned,
    normed,
    inner,
    halo,
    slot_of,
    weight_of,
    ranks,
    picked,
    expert_ref,
    mgain_ref,
    scale_ref,
    egain_ref,
    routes_t_ref,
    rw_t_ref,
    w_sem,
    in_sem,
    send_sem,
    ring_sem,
    disp_send,
    disp_sem,
    back_send,
    back_sem,
    halo_send,
    halo_sem,
):
    ep, tp = lax.axis_index("ep"), lax.axis_index("tp")
    n_ep = lax.axis_size("ep")
    n_z = n_ep // 2
    rows = mixer_hbm.shape[0]
    slots = n_ep * CAP
    z, core = ep // 2, ep % 2
    y, x = tp // SIDE, tp % SIDE
    yp, ym, xp, xm = (y + 1) % SIDE, (y + 3) % SIDE, (x + 1) % SIDE, (x + 3) % SIDE
    to_yp, to_ym = {"tp": yp * SIDE + x}, {"tp": ym * SIDE + x}
    to_xp, to_xm = {"tp": y * SIDE + xp}, {"tp": y * SIDE + xm}

    barrier = pltpu.get_barrier_semaphore()

    def peer_at(q, sign):
        dz = (q // 2 + 1) // 2 if (q // 2) % 2 == 1 else -(q // 2 // 2)
        other = (core + q % 2) % 2
        return {"ep": (z + sign * dz + n_z) % n_z * 2 + other}

    across_y, across_x = {"tp": (y + 2) % SIDE * SIDE + x}, {"tp": y * SIDE + (x + 2) % SIDE}
    plane = (to_yp, to_ym, to_xp, to_xm, across_y, across_x)
    for peer in [peer_at(q, 1) for q in range(n_ep - 1, 0, -1)] + list(plane):
        pl.semaphore_signal(barrier, inc=1, device_id=peer, device_id_type=MESH)

    own_rows = pltpu.make_async_copy(mixer_hbm, ring.at[y, x, 0:rows], in_sem.at[0])
    inputs = [
        pltpu.make_async_copy(routes_t_hbm, routes_t_ref, in_sem.at[1]),
        pltpu.make_async_copy(expert_hbm, expert_ref, in_sem.at[2]),
    ]
    others = [
        pltpu.make_async_copy(mgain_hbm, mgain_ref, in_sem.at[3]),
        pltpu.make_async_copy(scale_hbm, scale_ref, in_sem.at[4]),
        pltpu.make_async_copy(egain_hbm, egain_ref, in_sem.at[5]),
        pltpu.make_async_copy(rw_t_hbm, rw_t_ref, in_sem.at[6]),
    ]
    weights = others + [
        pltpu.make_async_copy(w_in_hbm, w_in, w_sem.at[0]),
        pltpu.make_async_copy(gate_hbm, w_gu.at[:, 0:128], w_sem.at[1]),
        pltpu.make_async_copy(up_hbm, w_gu.at[:, 128:256], w_sem.at[2]),
        pltpu.make_async_copy(w_mix_hbm, w_mix, w_sem.at[3]),
        pltpu.make_async_copy(down_hbm, w_down, w_sem.at[4]),
    ]
    for copy in inputs + [own_rows] + weights:
        copy.start()
    for copy in inputs:
        copy.wait()


    def step_of(q):
        j = q // 2
        return jnp.where(j % 2 == 1, (j + 1) // 2, 0 - j // 2)

    q_col = lax.broadcasted_iota(jnp.int32, (n_ep, 1), 0)

    def expert_at(q):
        other = (core + q % 2) % 2
        return (z + step_of(q) + n_z) % n_z * 2 + other

    e_col = expert_at(q_col)
    named = (routes_t_ref[0:1, :] == e_col) | (routes_t_ref[1:2, :] == e_col)
    r_iota = lax.broadcasted_iota(jnp.int32, (rows, rows), 0)
    c_iota = lax.broadcasted_iota(jnp.int32, (rows, rows), 1)
    before = jnp.where(r_iota < c_iota, 1.0, 0.0).astype(BF)
    rank = jnp.dot(
        jnp.where(named, 1.0, 0.0).astype(BF), before, preferred_element_type=F32
    )
    rank = jnp.where(named, rank, -1.0)
    ranks[...] = rank
    place = lax.broadcasted_iota(jnp.int32, (CAP, rows), 0).astype(F32)
    for g in range(n_ep // 8):
        hot = jnp.concatenate(
            [
                jnp.where(rank[q : q + 1, :] == place, 1.0, 0.0).astype(BF)
                for q in range(8 * g, 8 * g + 8)
            ],
            axis=0,
        )
        outgoing[8 * CAP * g : 8 * CAP * (g + 1), :] = jnp.dot(
            hot, expert_ref[...], preferred_element_type=F32
        ).astype(BF)
    ring[y, x, S0 * UNIT : S0 * UNIT + CAP, :] = outgoing[0:CAP, :]

    own_rows.wait()
    pl.semaphore_wait(barrier, n_ep - 1 + len(plane))

    def remote(src, dst, send, recv, device):
        pltpu.make_async_remote_copy(
            src_ref=src,
            dst_ref=dst,
            send_sem=send,
            recv_sem=recv,
            device_id=device,
            device_id_type=MESH,
        ).start()

    def await_bytes(ref, sem):
        pltpu.make_async_copy(ref, ref, sem).wait()

    def ring_copy(ref, sem, device):
        remote(ref, ref, send_sem, sem, device)

    def first_a(u):
        r = u * UNIT
        lo, hi = pl.ds(r, 64), pl.ds(r + 64, 64)
        ring_copy(ring.at[y, x, lo], ring_sem.at[u, 0, 0], to_xp)
        ring_copy(ring.at[y, x, hi], ring_sem.at[u, 1, 0], to_yp)
        ring_copy(ring.at[y, x, lo], ring_sem.at[u, 0, 0], to_xm)
        ring_copy(ring.at[y, x, hi], ring_sem.at[u, 1, 0], to_ym)

    def direct_a(u):
        r = u * UNIT
        lo, hi = pl.ds(r, 64), pl.ds(r + 64, 64)
        for to_x, to_y in ((to_xp, to_yp), (to_xm, to_ym), (across_x, across_y)):
            ring_copy(ring.at[y, x, lo], ring_sem.at[u, 0, 0], to_x)
            ring_copy(ring.at[y, x, hi], ring_sem.at[u, 1, 0], to_y)

    def second_a(u):
        r = u * UNIT
        await_bytes(ring.at[y, x, pl.ds(r, 128)], ring_sem.at[u, 0, 0])
        await_bytes(ring.at[y, x, pl.ds(r, 128)], ring_sem.at[u, 1, 0])
        ring_copy(ring.at[y, xm, pl.ds(r, 32)], ring_sem.at[u, 0, 1], to_xp)
        ring_copy(ring.at[ym, x, pl.ds(r + 64, 32)], ring_sem.at[u, 1, 1], to_yp)
        ring_copy(ring.at[y, xp, pl.ds(r + 32, 32)], ring_sem.at[u, 0, 1], to_xm)
        ring_copy(ring.at[yp, x, pl.ds(r + 96, 32)], ring_sem.at[u, 1, 1], to_ym)

    def first_b(u):
        r = u * UNIT
        lo, hi = pl.ds(r, 64), pl.ds(r + 64, 64)

        @pl.when(u < S0)
        def _():
            await_bytes(ring.at[y, 0:3, lo], ring_sem.at[u, 0, 0])
            await_bytes(ring.at[y, 0:3, lo], ring_sem.at[u, 1, 0])

        @pl.when(u >= S0)
        def _():
            await_bytes(ring.at[y, x, lo], ring_sem.at[u, 0, 1])
            await_bytes(ring.at[y, x, lo], ring_sem.at[u, 1, 1])

        ring_copy(ring.at[y, :, lo], ring_sem.at[u, 0, 2], to_yp)
        ring_copy(ring.at[:, x, hi], ring_sem.at[u, 1, 2], to_xp)
        ring_copy(ring.at[y, :, lo], ring_sem.at[u, 0, 2], to_ym)
        ring_copy(ring.at[:, x, hi], ring_sem.at[u, 1, 2], to_xm)

    def second_b(u):
        r = u * UNIT
        await_bytes(ring.at[y, :, pl.ds(r, 128)], ring_sem.at[u, 0, 2])
        await_bytes(ring.at[y, :, pl.ds(r, 128)], ring_sem.at[u, 1, 2])
        ring_copy(ring.at[ym, :, pl.ds(r, 32)], ring_sem.at[u, 0, 3], to_yp)
        ring_copy(ring.at[:, xm, pl.ds(r + 64, 32)], ring_sem.at[u, 1, 3], to_xp)
        ring_copy(ring.at[yp, :, pl.ds(r + 32, 32)], ring_sem.at[u, 0, 3], to_ym)
        ring_copy(ring.at[:, xp, pl.ds(r + 96, 32)], ring_sem.at[u, 1, 3], to_xm)

    def finished(u):
        r = u * UNIT
        await_bytes(ring.at[y, :, pl.ds(r, 64)], ring_sem.at[u, 0, 3])
        await_bytes(ring.at[y, :, pl.ds(r, 64)], ring_sem.at[u, 1, 3])

    for u in range(M0, M0 + rows // UNIT):
        direct_a(u)
    for q in range(1, n_ep):
        remote(
            outgoing.at[q * CAP : (q + 1) * CAP],
            ring.at[y, x, S0 * UNIT + q * CAP : S0 * UNIT + (q + 1) * CAP],
            disp_send,
            disp_sem.at[q // 8],
            peer_at(q, 1),
        )

    def place_results():
        e_at = expert_at(q_col)
        base = q_col.astype(F32) * float(CAP)
        for k in range(2):
            mine = routes_t_ref[k : k + 1, :] == e_at
            at = jnp.sum(jnp.where(mine, ranks[...] + base, 0.0), axis=0, keepdims=True)
            part = slice(k * rows, (k + 1) * rows)
            slot_of[part, :] = jnp.broadcast_to(at, (128, rows)).T
            weight_of[part, :] = jnp.broadcast_to(rw_t_ref[k : k + 1, :], (128, rows)).T

    picked[...] = jnp.zeros_like(picked)

    def layer_norm(u, gain_ref):
        def block(b, carry):
            r = pl.ds(u * UNIT + b * 32, 32)

            def piece(p):
                return ring[p // SIDE, p % SIDE, r, :].astype(F32)

            n = SIDE * SIDE
            total = piece(0)
            for p in range(1, n):
                total = total + piece(p)
            mean = jnp.sum(total, axis=1, keepdims=True) * (1.0 / (n * 128))
            square = None
            for p in range(n):
                d = piece(p) - mean
                square = d * d if square is None else square + d * d
            var = jnp.sum(square, axis=1, keepdims=True) * (1.0 / (n * 128))
            inv = lax.rsqrt(var + EPS)
            for p in range(n):
                normed[pl.ds(b * 32, 32), p * 128 : (p + 1) * 128] = (
                    (piece(p) - mean) * inv * gain_ref[p : p + 1, :]
                ).astype(BF)
            return carry

        lax.fori_loop(0, UNIT // 32, block, 0)

    def wide(u):
        r = pl.ds(u * UNIT, UNIT)
        return jnp.concatenate(
            [ring[p // SIDE, p % SIDE, r, :] for p in range(SIDE * SIDE)], axis=1
        )

    def mixer_unit(u):
        layer_norm(u, mgain_ref)
        inner[pl.ds((u - M0) * UNIT, UNIT), :] = jnp.dot(
            normed[...], w_in[...], preferred_element_type=F32
        ).astype(BF)

    def slot_unit(u):
        layer_norm(u, egain_ref)
        both = jnp.dot(normed[...], w_gu[...], preferred_element_type=F32)
        gate, up = both[:, 0:128], both[:, 128:256]
        hidden = gate / (1.0 + jnp.exp(-gate)) * up
        turn = (u - S0 + SLOT_UNITS - TURN) % SLOT_UNITS
        ring[y, x, pl.ds((turn + H0) * UNIT, UNIT), :] = hidden.astype(BF)

    def pooled_unit(u):
        out[pl.ds((u - P0) * UNIT, UNIT), :] = jnp.dot(
            wide(u), w_mix[...], preferred_element_type=F32
        ).astype(BF)

    def hidden_unit(u):
        turn = (u - H0 + TURN) % SLOT_UNITS
        back[pl.ds(turn * UNIT, UNIT), :] = jnp.dot(
            wide(u), w_down[...], preferred_element_type=F32
        ).astype(BF)

    def halo_out():
        remote(
            inner.at[rows - 16 : rows],
            halo.at[0:16],
            halo_send,
            halo_sem.at[0],
            {"ep": (ep + 1) % n_ep},
        )
        remote(
            inner.at[0:16],
            halo.at[16:32],
            halo_send,
            halo_sem.at[1],
            {"ep": (ep + n_ep - 1) % n_ep},
        )

    def pool():
        await_bytes(halo.at[0:16], halo_sem.at[0])
        await_bytes(halo.at[16:32], halo_sem.at[1])
        low = jnp.where(ep > 0, halo[8:16, :].astype(F32), 0.0)
        high = jnp.where(ep < n_ep - 1, halo[16:24, :].astype(F32), 0.0)
        values = inner[...].astype(F32)
        ext = jnp.concatenate([low, values, high], axis=0)
        two = ext[0 : rows + 15, :] + ext[1 : rows + 16, :]
        four = two[0 : rows + 13, :] + two[2 : rows + 15, :]
        eight = four[0 : rows + 9, :] + four[4 : rows + 13, :]
        sixteen = eight[0 : rows + 1, :] + eight[8 : rows + 9, :]
        total = jnp.where(
            y == 0,
            two[7 : 7 + rows, :],
            jnp.where(
                y == 1,
                four[6 : 6 + rows, :],
                jnp.where(y == 2, eight[4 : 4 + rows, :], sixteen[0:rows, :]),
            ),
        )
        reach = jnp.where(y == 0, 1, jnp.where(y == 1, 2, jnp.where(y == 2, 4, 8)))
        token = ep * rows + lax.broadcasted_iota(jnp.int32, (rows, 128), 0)
        count = jnp.minimum(token + reach, n_ep * rows) - jnp.maximum(token - reach, 0)
        result = (total / count.astype(F32) - values) * scale_ref[...]
        ring[y, x, P0 * UNIT : P0 * UNIT + rows, :] = result.astype(BF)

    def send_back(g):
        for q in range(8 * g, 8 * g + 8):
            part = slice(q * CAP, (q + 1) * CAP)
            if q == 0:
                returned[part, :] = back[part, :]
            else:
                remote(
                    back.at[part], returned.at[part], back_send, back_sem.at[g], peer_at(q, -1)
                )

    group = 8 * CAP
    lane = lax.broadcasted_iota(jnp.int32, (2 * rows, 128), 1).astype(F32)

    def combine(g):
        count = group if g > 0 else group - CAP
        await_bytes(returned.at[0:count], back_sem.at[g])
        where = slot_of[...]
        hot = jnp.concatenate(
            [
                jnp.where(where == lane + float(g * group + c * 128), 1.0, 0.0).astype(BF)
                for c in range(group // 128)
            ],
            axis=1,
        )
        picked[...] += jnp.dot(
            hot, returned[g * group : (g + 1) * group, :], preferred_element_type=F32
        )

    n_groups = n_ep // 8

    def sends(u):
        return ((u >= M0) & (u < M0 + rows // UNIT)) | ((u >= S0) & (u < UNITS))

    def step(i, carry):
        for lag, stage in ((B2, second_b), (B1, first_b), (A2, second_a)):
            u = i - lag

            @pl.when((u >= S0) & (u < UNITS) if stage is second_a else sends(u))
            def _():
                stage(u)

        for g in range(n_groups):

            @pl.when(i == S0 + 3 * g)
            def _():
                count = group if g > 0 else group - CAP
                await_bytes(ring.at[y, x, 0:count], disp_sem.at[g])

        @pl.when((i >= S0) & (i < UNITS))
        def _():
            first_a(i)

        u = i - DONE

        @pl.when(u == UNITS - 2)
        def _():
            combine(0)
            out[rows : 2 * rows, :] = (
                picked[0:rows, :] * weight_of[0:rows, :]
                + picked[rows : 2 * rows, :] * weight_of[rows : 2 * rows, :]
            ).astype(BF)

        @pl.when(sends(u))
        def _():
            finished(u)

        @pl.when(u == S0 + 2)
        def _():
            place_results()

        @pl.when(u == M0)
        def _():
            for copy in weights:
                copy.wait()

        @pl.when((u >= M0) & (u < M0 + rows // UNIT))
        def _():
            mixer_unit(u)

        @pl.when(u == M0 + rows // UNIT - 1)
        def _():
            halo_out()

        @pl.when(u == M0 + rows // UNIT + 2)
        def _():
            pool()

        @pl.when((u >= S0) & (u < H0))
        def _():
            slot_unit(u)

        @pl.when(u >= P0)
        def _():
            pooled_unit(u)

        @pl.when((u >= H0) & (u < P0))
        def _():
            hidden_unit(u)

        for g in range(n_groups):

            @pl.when(u == H0 + 3 * g + 2)
            def _():
                if g > 0:
                    combine(g)
                send_back((g + 1) % n_groups)

        return carry

    lax.fori_loop(B1, UNITS + DONE, step, 0)
    sent = (SIDE * SIDE - 1) * (2 * rows + 2 * slots) // (SIDE * SIDE)
    await_bytes(ring.at[:, :, 0:sent], send_sem)
    await_bytes(outgoing.at[0 : slots - CAP], disp_send)
    await_bytes(back.at[0 : slots - CAP], back_send)
    await_bytes(inner.at[0:32], halo_send)


def on_device(
    mixer_rows,
    expert_rows,
    mixer_gain,
    pool_scale,
    w_in,
    w_mix_out,
    expert_gain,
    expert_gate,
    expert_up,
    expert_down,
    routes,
    route_weight,
):
    rows, feats = mixer_rows.shape
    n_ep = lax.axis_size("ep")
    depth = w_in.shape[0]
    vmem = pl.BlockSpec(memory_space=pltpu.VMEM)
    hbm = pl.BlockSpec(memory_space=pl.ANY)
    slots = n_ep * CAP
    both = pl.pallas_call(
        kernel,
        name="mixer_and_experts",
        out_shape=jax.ShapeDtypeStruct((2 * rows, feats), BF),
        in_specs=[hbm] * 12,
        out_specs=vmem,
        scratch_shapes=[
            pltpu.VMEM((SIDE, SIDE, UNITS * UNIT, feats), BF),
            pltpu.VMEM((depth, 128), BF),
            pltpu.VMEM((depth, 128), BF),
            pltpu.VMEM((depth, 256), BF),
            pltpu.VMEM((depth, 128), BF),
            pltpu.VMEM((slots, feats), BF),
            pltpu.VMEM((slots, feats), BF),
            pltpu.VMEM((slots, feats), BF),
            pltpu.VMEM((UNIT, depth), BF),
            pltpu.VMEM((rows, feats), BF),
            pltpu.VMEM((32, feats), BF),
            pltpu.VMEM((2 * rows, 128), F32),
            pltpu.VMEM((2 * rows, 128), F32),
            pltpu.VMEM((n_ep, rows), F32),
            pltpu.VMEM((2 * rows, feats), F32),
            pltpu.VMEM((rows, feats), BF),
            pltpu.VMEM((depth // 128, 128), F32),
            pltpu.VMEM((1, feats), F32),
            pltpu.VMEM((depth // 128, 128), F32),
            pltpu.VMEM((2, rows), jnp.int32),
            pltpu.VMEM((2, rows), F32),
            pltpu.SemaphoreType.DMA((5,)),
            pltpu.SemaphoreType.DMA((7,)),
            pltpu.SemaphoreType.DMA,
            pltpu.SemaphoreType.DMA((UNITS, 2, 4)),
            pltpu.SemaphoreType.DMA,
            pltpu.SemaphoreType.DMA((n_ep // 8,)),
            pltpu.SemaphoreType.DMA,
            pltpu.SemaphoreType.DMA((n_ep // 8,)),
            pltpu.SemaphoreType.DMA,
            pltpu.SemaphoreType.DMA((2,)),
        ],
        compiler_params=pltpu.CompilerParams(
            collective_id=0, has_side_effects=True, vmem_limit_bytes=60 * 1024 * 1024
        ),
    )(
        mixer_rows,
        expert_rows,
        mixer_gain.reshape(-1, 128),
        pool_scale.reshape(1, -1),
        expert_gain.reshape(-1, 128),
        routes.T,
        route_weight.T,
        w_in,
        w_mix_out,
        expert_gate[0],
        expert_up[0],
        expert_down[0],
    )
    return both[0:rows], both[rows:]


def solution(mesh):
    return jax.shard_map(
        on_device,
        mesh=mesh,
        in_specs=(
            P("ep", "tp"),
            P("ep", "tp"),
            P(),
            P("tp"),
            P(None, "tp"),
            P(None, "tp"),
            P(),
            P("ep", None, "tp"),
            P("ep", None, "tp"),
            P("ep", None, "tp"),
            P("ep", None),
            P("ep", None),
        ),
        out_specs=(P("ep", "tp"), P("ep", "tp")),
        check_vma=False,
    )
```

```python
import jax
import jax.numpy as jnp
from jax import lax
from jax.experimental import pallas as pl
from jax.experimental.pallas import tpu as pltpu
from jax.sharding import PartitionSpec as P

MESH = pl.DeviceIdType.MESH
EPS = 1e-05
UNIT = 128
SLOT_UNITS, TURN = 12, 3
CAP = 48
SIDE = 4
M0, S0, H0, P0, UNITS = 0, 4, 16, 28, 32
A2, B1, B2, DONE = 2, 4, 6, 8
BF, F32 = jnp.bfloat16, jnp.float32


def kernel(
    mixer_hbm,
    expert_hbm,
    mgain_hbm,
    scale_hbm,
    egain_hbm,
    routes_t_hbm,
    rw_t_hbm,
    w_in_hbm,
    w_mix_hbm,
    gate_hbm,
    up_hbm,
    down_hbm,
    out,
    ring,
    w_in,
    w_mix,
    w_gu,
    w_down,
    outgoing,
    back,
    returned,
    normed,
    inner,
    halo,
    slot_of,
    weight_of,
    ranks,
    picked,
    expert_ref,
    mgain_ref,
    scale_ref,
    egain_ref,
    routes_t_ref,
    rw_t_ref,
    w_sem,
    in_sem,
    send_sem,
    ring_sem,
    disp_send,
    disp_sem,
    back_send,
    back_sem,
    halo_send,
    halo_sem,
):
    ep, tp = lax.axis_index("ep"), lax.axis_index("tp")
    n_ep = lax.axis_size("ep")
    n_z = n_ep // 2
    rows = mixer_hbm.shape[0]
    slots = n_ep * CAP
    z, core = ep // 2, ep % 2
    y, x = tp // SIDE, tp % SIDE
    yp, ym, xp, xm = (y + 1) % SIDE, (y + 3) % SIDE, (x + 1) % SIDE, (x + 3) % SIDE
    to_yp, to_ym = {"tp": yp * SIDE + x}, {"tp": ym * SIDE + x}
    to_xp, to_xm = {"tp": y * SIDE + xp}, {"tp": y * SIDE + xm}

    barrier = pltpu.get_barrier_semaphore()

    def peer_at(q, sign):
        dz = (q // 2 + 1) // 2 if (q // 2) % 2 == 1 else -(q // 2 // 2)
        other = (core + q % 2) % 2
        return {"ep": (z + sign * dz + n_z) % n_z * 2 + other}

    across_y, across_x = {"tp": (y + 2) % SIDE * SIDE + x}, {"tp": y * SIDE + (x + 2) % SIDE}
    plane = (to_yp, to_ym, to_xp, to_xm, across_y, across_x)
    for peer in [peer_at(q, 1) for q in range(n_ep - 1, 0, -1)] + list(plane):
        pl.semaphore_signal(barrier, inc=1, device_id=peer, device_id_type=MESH)

    own_rows = pltpu.make_async_copy(mixer_hbm, ring.at[y, x, 0:rows], in_sem.at[0])
    inputs = [
        pltpu.make_async_copy(routes_t_hbm, routes_t_ref, in_sem.at[1]),
        pltpu.make_async_copy(expert_hbm, expert_ref, in_sem.at[2]),
    ]
    others = [
        pltpu.make_async_copy(mgain_hbm, mgain_ref, in_sem.at[3]),
        pltpu.make_async_copy(scale_hbm, scale_ref, in_sem.at[4]),
        pltpu.make_async_copy(egain_hbm, egain_ref, in_sem.at[5]),
        pltpu.make_async_copy(rw_t_hbm, rw_t_ref, in_sem.at[6]),
    ]
    weights = others + [
        pltpu.make_async_copy(w_in_hbm, w_in, w_sem.at[0]),
        pltpu.make_async_copy(gate_hbm, w_gu.at[:, 0:128], w_sem.at[1]),
        pltpu.make_async_copy(up_hbm, w_gu.at[:, 128:256], w_sem.at[2]),
        pltpu.make_async_copy(w_mix_hbm, w_mix, w_sem.at[3]),
        pltpu.make_async_copy(down_hbm, w_down, w_sem.at[4]),
    ]
    for copy in inputs + [own_rows] + weights:
        copy.start()
    for copy in inputs:
        copy.wait()


    def step_of(q):
        j = q // 2
        return jnp.where(j % 2 == 1, (j + 1) // 2, 0 - j // 2)

    q_col = lax.broadcasted_iota(jnp.int32, (n_ep, 1), 0)

    def expert_at(q):
        other = (core + q % 2) % 2
        return (z + step_of(q) + n_z) % n_z * 2 + other

    e_col = expert_at(q_col)
    named = (routes_t_ref[0:1, :] == e_col) | (routes_t_ref[1:2, :] == e_col)
    r_iota = lax.broadcasted_iota(jnp.int32, (rows, rows), 0)
    c_iota = lax.broadcasted_iota(jnp.int32, (rows, rows), 1)
    before = jnp.where(r_iota < c_iota, 1.0, 0.0).astype(BF)
    rank = jnp.dot(
        jnp.where(named, 1.0, 0.0).astype(BF), before, preferred_element_type=F32
    )
    rank = jnp.where(named, rank, -1.0)
    ranks[...] = rank
    place = lax.broadcasted_iota(jnp.int32, (CAP, rows), 0).astype(F32)
    for g in range(n_ep // 8):
        hot = jnp.concatenate(
            [
                jnp.where(rank[q : q + 1, :] == place, 1.0, 0.0).astype(BF)
                for q in range(8 * g, 8 * g + 8)
            ],
            axis=0,
        )
        outgoing[8 * CAP * g : 8 * CAP * (g + 1), :] = jnp.dot(
            hot, expert_ref[...], preferred_element_type=F32
        ).astype(BF)
    ring[y, x, S0 * UNIT : S0 * UNIT + CAP, :] = outgoing[0:CAP, :]

    own_rows.wait()
    pl.semaphore_wait(barrier, n_ep - 1 + len(plane))

    def remote(src, dst, send, recv, device):
        pltpu.make_async_remote_copy(
            src_ref=src,
            dst_ref=dst,
            send_sem=send,
            recv_sem=recv,
            device_id=device,
            device_id_type=MESH,
        ).start()

    def await_bytes(ref, sem):
        pltpu.make_async_copy(ref, ref, sem).wait()

    def ring_copy(ref, sem, device):
        remote(ref, ref, send_sem, sem, device)

    def first_a(u):
        r = u * UNIT
        lo, hi = pl.ds(r, 64), pl.ds(r + 64, 64)
        ring_copy(ring.at[y, x, lo], ring_sem.at[u, 0, 0], to_xp)
        ring_copy(ring.at[y, x, hi], ring_sem.at[u, 1, 0], to_yp)
        ring_copy(ring.at[y, x, lo], ring_sem.at[u, 0, 0], to_xm)
        ring_copy(ring.at[y, x, hi], ring_sem.at[u, 1, 0], to_ym)

    def direct_a(u):
        r = u * UNIT
        lo, hi = pl.ds(r, 64), pl.ds(r + 64, 64)
        for to_x, to_y in ((to_xp, to_yp), (to_xm, to_ym), (across_x, across_y)):
            ring_copy(ring.at[y, x, lo], ring_sem.at[u, 0, 0], to_x)
            ring_copy(ring.at[y, x, hi], ring_sem.at[u, 1, 0], to_y)

    def second_a(u):
        r = u * UNIT
        await_bytes(ring.at[y, x, pl.ds(r, 128)], ring_sem.at[u, 0, 0])
        await_bytes(ring.at[y, x, pl.ds(r, 128)], ring_sem.at[u, 1, 0])
        ring_copy(ring.at[y, xm, pl.ds(r, 32)], ring_sem.at[u, 0, 1], to_xp)
        ring_copy(ring.at[ym, x, pl.ds(r + 64, 32)], ring_sem.at[u, 1, 1], to_yp)
        ring_copy(ring.at[y, xp, pl.ds(r + 32, 32)], ring_sem.at[u, 0, 1], to_xm)
        ring_copy(ring.at[yp, x, pl.ds(r + 96, 32)], ring_sem.at[u, 1, 1], to_ym)

    def first_b(u):
        r = u * UNIT
        lo, hi = pl.ds(r, 64), pl.ds(r + 64, 64)

        @pl.when(u < S0)
        def _():
            await_bytes(ring.at[y, 0:3, lo], ring_sem.at[u, 0, 0])
            await_bytes(ring.at[y, 0:3, lo], ring_sem.at[u, 1, 0])

        @pl.when(u >= S0)
        def _():
            await_bytes(ring.at[y, x, lo], ring_sem.at[u, 0, 1])
            await_bytes(ring.at[y, x, lo], ring_sem.at[u, 1, 1])

        ring_copy(ring.at[y, :, lo], ring_sem.at[u, 0, 2], to_yp)
        ring_copy(ring.at[:, x, hi], ring_sem.at[u, 1, 2], to_xp)
        ring_copy(ring.at[y, :, lo], ring_sem.at[u, 0, 2], to_ym)
        ring_copy(ring.at[:, x, hi], ring_sem.at[u, 1, 2], to_xm)

    def second_b(u):
        r = u * UNIT
        await_bytes(ring.at[y, :, pl.ds(r, 128)], ring_sem.at[u, 0, 2])
        await_bytes(ring.at[y, :, pl.ds(r, 128)], ring_sem.at[u, 1, 2])
        ring_copy(ring.at[ym, :, pl.ds(r, 32)], ring_sem.at[u, 0, 3], to_yp)
        ring_copy(ring.at[:, xm, pl.ds(r + 64, 32)], ring_sem.at[u, 1, 3], to_xp)
        ring_copy(ring.at[yp, :, pl.ds(r + 32, 32)], ring_sem.at[u, 0, 3], to_ym)
        ring_copy(ring.at[:, xp, pl.ds(r + 96, 32)], ring_sem.at[u, 1, 3], to_xm)

    def finished(u):
        r = u * UNIT
        await_bytes(ring.at[y, :, pl.ds(r, 64)], ring_sem.at[u, 0, 3])
        await_bytes(ring.at[y, :, pl.ds(r, 64)], ring_sem.at[u, 1, 3])

    for u in range(M0, M0 + rows // UNIT):
        direct_a(u)
    for q in range(1, n_ep):
        remote(
            outgoing.at[q * CAP : (q + 1) * CAP],
            ring.at[y, x, S0 * UNIT + q * CAP : S0 * UNIT + (q + 1) * CAP],
            disp_send,
            disp_sem.at[q // 8 * 3 + q % 8 // 3],
            peer_at(q, 1),
        )

    def place_results():
        e_at = expert_at(q_col)
        base = q_col.astype(F32) * float(CAP)
        for k in range(2):
            mine = routes_t_ref[k : k + 1, :] == e_at
            at = jnp.sum(jnp.where(mine, ranks[...] + base, 0.0), axis=0, keepdims=True)
            part = slice(k * rows, (k + 1) * rows)
            slot_of[part, :] = jnp.broadcast_to(at, (128, rows)).T
            weight_of[part, :] = jnp.broadcast_to(rw_t_ref[k : k + 1, :], (128, rows)).T

    picked[...] = jnp.zeros_like(picked)

    def layer_norm(u, gain_ref):
        def block(b, carry):
            r = pl.ds(u * UNIT + b * 32, 32)

            def piece(p):
                return ring[p // SIDE, p % SIDE, r, :].astype(F32)

            n = SIDE * SIDE
            total = piece(0)
            for p in range(1, n):
                total = total + piece(p)
            mean = jnp.sum(total, axis=1, keepdims=True) * (1.0 / (n * 128))
            square = None
            for p in range(n):
                d = piece(p) - mean
                square = d * d if square is None else square + d * d
            var = jnp.sum(square, axis=1, keepdims=True) * (1.0 / (n * 128))
            inv = lax.rsqrt(var + EPS)
            for p in range(n):
                normed[pl.ds(b * 32, 32), p * 128 : (p + 1) * 128] = (
                    (piece(p) - mean) * inv * gain_ref[p : p + 1, :]
                ).astype(BF)
            return carry

        lax.fori_loop(0, UNIT // 32, block, 0)

    def wide(u):
        r = pl.ds(u * UNIT, UNIT)
        return jnp.concatenate(
            [ring[p // SIDE, p % SIDE, r, :] for p in range(SIDE * SIDE)], axis=1
        )

    def mixer_unit(u):
        layer_norm(u, mgain_ref)
        inner[pl.ds((u - M0) * UNIT, UNIT), :] = jnp.dot(
            normed[...], w_in[...], preferred_element_type=F32
        ).astype(BF)

    def slot_unit(u):
        layer_norm(u, egain_ref)
        both = jnp.dot(normed[...], w_gu[...], preferred_element_type=F32)
        gate, up = both[:, 0:128], both[:, 128:256]
        hidden = gate / (1.0 + jnp.exp(-gate)) * up
        turn = (u - S0 + SLOT_UNITS - TURN) % SLOT_UNITS
        ring[y, x, pl.ds((turn + H0) * UNIT, UNIT), :] = hidden.astype(BF)

    def pooled_unit(u):
        out[pl.ds((u - P0) * UNIT, UNIT), :] = jnp.dot(
            wide(u), w_mix[...], preferred_element_type=F32
        ).astype(BF)

    def hidden_unit(u):
        turn = (u - H0 + TURN) % SLOT_UNITS
        back[pl.ds(turn * UNIT, UNIT), :] = jnp.dot(
            wide(u), w_down[...], preferred_element_type=F32
        ).astype(BF)

    def halo_out():
        remote(
            inner.at[rows - 16 : rows],
            halo.at[0:16],
            halo_send,
            halo_sem.at[0],
            {"ep": (ep + 1) % n_ep},
        )
        remote(
            inner.at[0:16],
            halo.at[16:32],
            halo_send,
            halo_sem.at[1],
            {"ep": (ep + n_ep - 1) % n_ep},
        )

    def pool():
        await_bytes(halo.at[0:16], halo_sem.at[0])
        await_bytes(halo.at[16:32], halo_sem.at[1])
        low = jnp.where(ep > 0, halo[8:16, :].astype(F32), 0.0)
        high = jnp.where(ep < n_ep - 1, halo[16:24, :].astype(F32), 0.0)
        values = inner[...].astype(F32)
        ext = jnp.concatenate([low, values, high], axis=0)
        two = ext[0 : rows + 15, :] + ext[1 : rows + 16, :]
        four = two[0 : rows + 13, :] + two[2 : rows + 15, :]
        eight = four[0 : rows + 9, :] + four[4 : rows + 13, :]
        sixteen = eight[0 : rows + 1, :] + eight[8 : rows + 9, :]
        total = jnp.where(
            y == 0,
            two[7 : 7 + rows, :],
            jnp.where(
                y == 1,
                four[6 : 6 + rows, :],
                jnp.where(y == 2, eight[4 : 4 + rows, :], sixteen[0:rows, :]),
            ),
        )
        reach = jnp.where(y == 0, 1, jnp.where(y == 1, 2, jnp.where(y == 2, 4, 8)))
        token = ep * rows + lax.broadcasted_iota(jnp.int32, (rows, 128), 0)
        count = jnp.minimum(token + reach, n_ep * rows) - jnp.maximum(token - reach, 0)
        result = (total / count.astype(F32) - values) * scale_ref[...]
        ring[y, x, P0 * UNIT : P0 * UNIT + rows, :] = result.astype(BF)

    def send_back(g):
        for q in range(8 * g, 8 * g + 8):
            part = slice(q * CAP, (q + 1) * CAP)
            if q == 0:
                returned[part, :] = back[part, :]
            else:
                remote(
                    back.at[part], returned.at[part], back_send, back_sem.at[g], peer_at(q, -1)
                )

    group = 8 * CAP
    lane = lax.broadcasted_iota(jnp.int32, (2 * rows, 128), 1).astype(F32)

    def combine(g):
        count = group if g > 0 else group - CAP
        await_bytes(returned.at[0:count], back_sem.at[g])
        where = slot_of[...]
        hot = jnp.concatenate(
            [
                jnp.where(where == lane + float(g * group + c * 128), 1.0, 0.0).astype(BF)
                for c in range(group // 128)
            ],
            axis=1,
        )
        picked[...] += jnp.dot(
            hot, returned[g * group : (g + 1) * group, :], preferred_element_type=F32
        )

    n_groups = n_ep // 8

    def sends(u):
        return ((u >= M0) & (u < M0 + rows // UNIT)) | ((u >= S0) & (u < UNITS))

    def step(i, carry):
        for lag, stage in ((B2, second_b), (B1, first_b), (A2, second_a)):
            u = i - lag

            @pl.when((u >= S0) & (u < UNITS) if stage is second_a else sends(u))
            def _():
                stage(u)

        k = i - S0
        for first, count in ((0, 3), (1, 3), (2, 2)):

            @pl.when((k > 0) & (k < SLOT_UNITS) & (k % 3 == first))
            def _():
                await_bytes(ring.at[y, x, 0 : count * CAP], disp_sem.at[k])

        @pl.when(k == 0)
        def _():
            await_bytes(ring.at[y, x, 0 : 2 * CAP], disp_sem.at[0])

        @pl.when((i >= S0) & (i < UNITS))
        def _():
            first_a(i)

        u = i - DONE

        @pl.when(u == UNITS - 2)
        def _():
            combine(0)
            out[rows : 2 * rows, :] = (
                picked[0:rows, :] * weight_of[0:rows, :]
                + picked[rows : 2 * rows, :] * weight_of[rows : 2 * rows, :]
            ).astype(BF)

        @pl.when(sends(u))
        def _():
            finished(u)

        @pl.when(u == S0 + 2)
        def _():
            place_results()

        @pl.when(u == M0)
        def _():
            for copy in weights:
                copy.wait()

        @pl.when((u >= M0) & (u < M0 + rows // UNIT))
        def _():
            mixer_unit(u)

        @pl.when(u == M0 + rows // UNIT - 1)
        def _():
            halo_out()

        @pl.when(u == M0 + rows // UNIT + 2)
        def _():
            pool()

        @pl.when((u >= S0) & (u < H0))
        def _():
            slot_unit(u)

        @pl.when(u >= P0)
        def _():
            pooled_unit(u)

        @pl.when((u >= H0) & (u < P0))
        def _():
            hidden_unit(u)

        for g in range(n_groups):

            @pl.when(u == H0 + 3 * g + 2)
            def _():
                if g > 0:
                    combine(g)
                send_back((g + 1) % n_groups)

        return carry

    lax.fori_loop(B1, UNITS + DONE, step, 0)
    sent = (SIDE * SIDE - 1) * (2 * rows + 2 * slots) // (SIDE * SIDE)
    await_bytes(ring.at[:, :, 0:sent], send_sem)
    await_bytes(outgoing.at[0 : slots - CAP], disp_send)
    await_bytes(back.at[0 : slots - CAP], back_send)
    await_bytes(inner.at[0:32], halo_send)


def on_device(
    mixer_rows,
    expert_rows,
    mixer_gain,
    pool_scale,
    w_in,
    w_mix_out,
    expert_gain,
    expert_gate,
    expert_up,
    expert_down,
    routes,
    route_weight,
):
    rows, feats = mixer_rows.shape
    n_ep = lax.axis_size("ep")
    depth = w_in.shape[0]
    vmem = pl.BlockSpec(memory_space=pltpu.VMEM)
    hbm = pl.BlockSpec(memory_space=pl.ANY)
    slots = n_ep * CAP
    both = pl.pallas_call(
        kernel,
        name="mixer_and_experts",
        out_shape=jax.ShapeDtypeStruct((2 * rows, feats), BF),
        in_specs=[hbm] * 12,
        out_specs=vmem,
        scratch_shapes=[
            pltpu.VMEM((SIDE, SIDE, UNITS * UNIT, feats), BF),
            pltpu.VMEM((depth, 128), BF),
            pltpu.VMEM((depth, 128), BF),
            pltpu.VMEM((depth, 256), BF),
            pltpu.VMEM((depth, 128), BF),
            pltpu.VMEM((slots, feats), BF),
            pltpu.VMEM((slots, feats), BF),
            pltpu.VMEM((slots, feats), BF),
            pltpu.VMEM((UNIT, depth), BF),
            pltpu.VMEM((rows, feats), BF),
            pltpu.VMEM((32, feats), BF),
            pltpu.VMEM((2 * rows, 128), F32),
            pltpu.VMEM((2 * rows, 128), F32),
            pltpu.VMEM((n_ep, rows), F32),
            pltpu.VMEM((2 * rows, feats), F32),
            pltpu.VMEM((rows, feats), BF),
            pltpu.VMEM((depth // 128, 128), F32),
            pltpu.VMEM((1, feats), F32),
            pltpu.VMEM((depth // 128, 128), F32),
            pltpu.VMEM((2, rows), jnp.int32),
            pltpu.VMEM((2, rows), F32),
            pltpu.SemaphoreType.DMA((5,)),
            pltpu.SemaphoreType.DMA((7,)),
            pltpu.SemaphoreType.DMA,
            pltpu.SemaphoreType.DMA((UNITS, 2, 4)),
            pltpu.SemaphoreType.DMA,
            pltpu.SemaphoreType.DMA((SLOT_UNITS,)),
            pltpu.SemaphoreType.DMA,
            pltpu.SemaphoreType.DMA((n_ep // 8,)),
            pltpu.SemaphoreType.DMA,
            pltpu.SemaphoreType.DMA((2,)),
        ],
        compiler_params=pltpu.CompilerParams(
            collective_id=0, has_side_effects=True, vmem_limit_bytes=60 * 1024 * 1024
        ),
    )(
        mixer_rows,
        expert_rows,
        mixer_gain.reshape(-1, 128),
        pool_scale.reshape(1, -1),
        expert_gain.reshape(-1, 128),
        routes.T,
        route_weight.T,
        w_in,
        w_mix_out,
        expert_gate[0],
        expert_up[0],
        expert_down[0],
    )
    return both[0:rows], both[rows:]


def solution(mesh):
    return jax.shard_map(
        on_device,
        mesh=mesh,
        in_specs=(
            P("ep", "tp"),
            P("ep", "tp"),
            P(),
            P("tp"),
            P(None, "tp"),
            P(None, "tp"),
            P(),
            P("ep", None, "tp"),
            P("ep", None, "tp"),
            P("ep", None, "tp"),
            P("ep", None),
            P("ep", None),
        ),
        out_specs=(P("ep", "tp"), P("ep", "tp")),
        check_vma=False,
    )
```

```python
import jax
import jax.numpy as jnp
from jax import lax
from jax.experimental import pallas as pl
from jax.experimental.pallas import tpu as pltpu
from jax.sharding import PartitionSpec as P

MESH = pl.DeviceIdType.MESH
EPS = 1e-05
UNIT = 128
SLOT_UNITS, TURN = 12, 3
CAP = 48
SIDE = 4
M0, S0, H0, P0, UNITS = 0, 4, 16, 28, 32
A2, B1, B2, DONE = 2, 4, 6, 8
BF, F32 = jnp.bfloat16, jnp.float32


def kernel(
    mixer_hbm,
    expert_hbm,
    mgain_hbm,
    scale_hbm,
    egain_hbm,
    routes_t_hbm,
    rw_t_hbm,
    w_in_hbm,
    w_mix_hbm,
    gate_hbm,
    up_hbm,
    down_hbm,
    out,
    ring,
    w_in,
    w_mix,
    w_gu,
    w_down,
    outgoing,
    back,
    returned,
    normed,
    inner,
    halo,
    slot_of,
    weight_of,
    ranks,
    picked,
    expert_ref,
    mgain_ref,
    scale_ref,
    egain_ref,
    routes_t_ref,
    rw_t_ref,
    w_sem,
    in_sem,
    send_sem,
    ring_sem,
    disp_send,
    disp_sem,
    back_send,
    back_sem,
    halo_send,
    halo_sem,
):
    ep, tp = lax.axis_index("ep"), lax.axis_index("tp")
    n_ep = lax.axis_size("ep")
    n_z = n_ep // 2
    rows = mixer_hbm.shape[0]
    slots = n_ep * CAP
    z, core = ep // 2, ep % 2
    y, x = tp // SIDE, tp % SIDE
    yp, ym, xp, xm = (y + 1) % SIDE, (y + 3) % SIDE, (x + 1) % SIDE, (x + 3) % SIDE
    to_yp, to_ym = {"tp": yp * SIDE + x}, {"tp": ym * SIDE + x}
    to_xp, to_xm = {"tp": y * SIDE + xp}, {"tp": y * SIDE + xm}

    barrier = pltpu.get_barrier_semaphore()

    def peer_at(q, sign):
        dz = (q // 2 + 1) // 2 if (q // 2) % 2 == 1 else -(q // 2 // 2)
        other = (core + q % 2) % 2
        return {"ep": (z + sign * dz + n_z) % n_z * 2 + other}

    across_y, across_x = {"tp": (y + 2) % SIDE * SIDE + x}, {"tp": y * SIDE + (x + 2) % SIDE}
    plane = (to_yp, to_ym, to_xp, to_xm, across_y, across_x)
    for peer in [peer_at(q, 1) for q in range(n_ep - 1, 0, -1)] + list(plane):
        pl.semaphore_signal(barrier, inc=1, device_id=peer, device_id_type=MESH)

    own_rows = pltpu.make_async_copy(mixer_hbm, ring.at[y, x, 0:rows], in_sem.at[0])
    inputs = [
        pltpu.make_async_copy(routes_t_hbm, routes_t_ref, in_sem.at[1]),
        pltpu.make_async_copy(expert_hbm, expert_ref, in_sem.at[2]),
    ]
    others = [
        pltpu.make_async_copy(mgain_hbm, mgain_ref, in_sem.at[3]),
        pltpu.make_async_copy(scale_hbm, scale_ref, in_sem.at[4]),
        pltpu.make_async_copy(egain_hbm, egain_ref, in_sem.at[5]),
        pltpu.make_async_copy(rw_t_hbm, rw_t_ref, in_sem.at[6]),
    ]
    weights = others + [
        pltpu.make_async_copy(w_in_hbm, w_in, w_sem.at[0]),
        pltpu.make_async_copy(gate_hbm, w_gu.at[:, 0:128], w_sem.at[1]),
        pltpu.make_async_copy(up_hbm, w_gu.at[:, 128:256], w_sem.at[2]),
        pltpu.make_async_copy(w_mix_hbm, w_mix, w_sem.at[3]),
        pltpu.make_async_copy(down_hbm, w_down, w_sem.at[4]),
    ]
    for copy in inputs + [own_rows] + weights:
        copy.start()
    for copy in inputs:
        copy.wait()


    def step_of(q):
        j = q // 2
        return jnp.where(j % 2 == 1, (j + 1) // 2, 0 - j // 2)

    q_col = lax.broadcasted_iota(jnp.int32, (n_ep, 1), 0)

    def expert_at(q):
        other = (core + q % 2) % 2
        return (z + step_of(q) + n_z) % n_z * 2 + other

    e_col = expert_at(q_col)
    named = (routes_t_ref[0:1, :] == e_col) | (routes_t_ref[1:2, :] == e_col)
    r_iota = lax.broadcasted_iota(jnp.int32, (rows, rows), 0)
    c_iota = lax.broadcasted_iota(jnp.int32, (rows, rows), 1)
    before = jnp.where(r_iota < c_iota, 1.0, 0.0).astype(BF)
    rank = jnp.dot(
        jnp.where(named, 1.0, 0.0).astype(BF), before, preferred_element_type=F32
    )
    rank = jnp.where(named, rank, -1.0)
    ranks[...] = rank
    place = lax.broadcasted_iota(jnp.int32, (CAP, rows), 0).astype(F32)
    for g in range(n_ep // 8):
        hot = jnp.concatenate(
            [
                jnp.where(rank[q : q + 1, :] == place, 1.0, 0.0).astype(BF)
                for q in range(8 * g, 8 * g + 8)
            ],
            axis=0,
        )
        outgoing[8 * CAP * g : 8 * CAP * (g + 1), :] = jnp.dot(
            hot, expert_ref[...], preferred_element_type=F32
        ).astype(BF)
    ring[y, x, S0 * UNIT : S0 * UNIT + CAP, :] = outgoing[0:CAP, :]

    own_rows.wait()
    pl.semaphore_wait(barrier, n_ep - 1 + len(plane))

    def remote(src, dst, send, recv, device):
        pltpu.make_async_remote_copy(
            src_ref=src,
            dst_ref=dst,
            send_sem=send,
            recv_sem=recv,
            device_id=device,
            device_id_type=MESH,
        ).start()

    def await_bytes(ref, sem):
        pltpu.make_async_copy(ref, ref, sem).wait()

    def ring_copy(ref, sem, device):
        remote(ref, ref, send_sem, sem, device)

    def first_a(u):
        r = u * UNIT
        lo, hi = pl.ds(r, 64), pl.ds(r + 64, 64)
        ring_copy(ring.at[y, x, lo], ring_sem.at[u, 0, 0], to_xp)
        ring_copy(ring.at[y, x, hi], ring_sem.at[u, 1, 0], to_yp)
        ring_copy(ring.at[y, x, lo], ring_sem.at[u, 0, 0], to_xm)
        ring_copy(ring.at[y, x, hi], ring_sem.at[u, 1, 0], to_ym)

    def direct_a(u):
        r = u * UNIT
        lo, hi = pl.ds(r, 64), pl.ds(r + 64, 64)
        for to_x, to_y in ((to_xp, to_yp), (to_xm, to_ym), (across_x, across_y)):
            ring_copy(ring.at[y, x, lo], ring_sem.at[u, 0, 0], to_x)
            ring_copy(ring.at[y, x, hi], ring_sem.at[u, 1, 0], to_y)

    def second_a(u):
        r = u * UNIT
        await_bytes(ring.at[y, x, pl.ds(r, 128)], ring_sem.at[u, 0, 0])
        await_bytes(ring.at[y, x, pl.ds(r, 128)], ring_sem.at[u, 1, 0])
        ring_copy(ring.at[y, xm, pl.ds(r, 32)], ring_sem.at[u, 0, 1], to_xp)
        ring_copy(ring.at[ym, x, pl.ds(r + 64, 32)], ring_sem.at[u, 1, 1], to_yp)
        ring_copy(ring.at[y, xp, pl.ds(r + 32, 32)], ring_sem.at[u, 0, 1], to_xm)
        ring_copy(ring.at[yp, x, pl.ds(r + 96, 32)], ring_sem.at[u, 1, 1], to_ym)

    def first_b(u):
        r = u * UNIT
        lo, hi = pl.ds(r, 64), pl.ds(r + 64, 64)

        @pl.when(u < S0)
        def _():
            await_bytes(ring.at[y, 0:3, lo], ring_sem.at[u, 0, 0])
            await_bytes(ring.at[y, 0:3, lo], ring_sem.at[u, 1, 0])

        @pl.when(u >= S0)
        def _():
            await_bytes(ring.at[y, x, lo], ring_sem.at[u, 0, 1])
            await_bytes(ring.at[y, x, lo], ring_sem.at[u, 1, 1])

        ring_copy(ring.at[y, :, lo], ring_sem.at[u, 0, 2], to_yp)
        ring_copy(ring.at[:, x, hi], ring_sem.at[u, 1, 2], to_xp)
        ring_copy(ring.at[y, :, lo], ring_sem.at[u, 0, 2], to_ym)
        ring_copy(ring.at[:, x, hi], ring_sem.at[u, 1, 2], to_xm)

    def second_b(u):
        r = u * UNIT
        await_bytes(ring.at[y, :, pl.ds(r, 128)], ring_sem.at[u, 0, 2])
        await_bytes(ring.at[y, :, pl.ds(r, 128)], ring_sem.at[u, 1, 2])
        ring_copy(ring.at[ym, :, pl.ds(r, 32)], ring_sem.at[u, 0, 3], to_yp)
        ring_copy(ring.at[:, xm, pl.ds(r + 64, 32)], ring_sem.at[u, 1, 3], to_xp)
        ring_copy(ring.at[yp, :, pl.ds(r + 32, 32)], ring_sem.at[u, 0, 3], to_ym)
        ring_copy(ring.at[:, xp, pl.ds(r + 96, 32)], ring_sem.at[u, 1, 3], to_xm)

    def finished(u):
        r = u * UNIT
        await_bytes(ring.at[y, :, pl.ds(r, 64)], ring_sem.at[u, 0, 3])
        await_bytes(ring.at[y, :, pl.ds(r, 64)], ring_sem.at[u, 1, 3])

    def dispatch(q):
        remote(
            outgoing.at[q * CAP : (q + 1) * CAP],
            ring.at[y, x, S0 * UNIT + q * CAP : S0 * UNIT + (q + 1) * CAP],
            disp_send,
            disp_sem.at[q // 8 * 3 + q % 8 // 3],
            peer_at(q, 1),
        )

    for q in range(1, 8):
        dispatch(q)
    for u in range(M0, M0 + rows // UNIT):
        direct_a(u)
    for q in range(8, n_ep):
        dispatch(q)

    def place_results():
        e_at = expert_at(q_col)
        base = q_col.astype(F32) * float(CAP)
        for k in range(2):
            mine = routes_t_ref[k : k + 1, :] == e_at
            at = jnp.sum(jnp.where(mine, ranks[...] + base, 0.0), axis=0, keepdims=True)
            part = slice(k * rows, (k + 1) * rows)
            slot_of[part, :] = jnp.broadcast_to(at, (128, rows)).T
            weight_of[part, :] = jnp.broadcast_to(rw_t_ref[k : k + 1, :], (128, rows)).T

    picked[...] = jnp.zeros_like(picked)

    def layer_norm(u, gain_ref):
        def block(b, carry):
            r = pl.ds(u * UNIT + b * 32, 32)

            def piece(p):
                return ring[p // SIDE, p % SIDE, r, :].astype(F32)

            n = SIDE * SIDE
            total = piece(0)
            for p in range(1, n):
                total = total + piece(p)
            mean = jnp.sum(total, axis=1, keepdims=True) * (1.0 / (n * 128))
            square = None
            for p in range(n):
                d = piece(p) - mean
                square = d * d if square is None else square + d * d
            var = jnp.sum(square, axis=1, keepdims=True) * (1.0 / (n * 128))
            inv = lax.rsqrt(var + EPS)
            for p in range(n):
                normed[pl.ds(b * 32, 32), p * 128 : (p + 1) * 128] = (
                    (piece(p) - mean) * inv * gain_ref[p : p + 1, :]
                ).astype(BF)
            return carry

        lax.fori_loop(0, UNIT // 32, block, 0)

    def wide(u):
        r = pl.ds(u * UNIT, UNIT)
        return jnp.concatenate(
            [ring[p // SIDE, p % SIDE, r, :] for p in range(SIDE * SIDE)], axis=1
        )

    def mixer_unit(u):
        layer_norm(u, mgain_ref)
        inner[pl.ds((u - M0) * UNIT, UNIT), :] = jnp.dot(
            normed[...], w_in[...], preferred_element_type=F32
        ).astype(BF)

    def slot_unit(u):
        layer_norm(u, egain_ref)
        both = jnp.dot(normed[...], w_gu[...], preferred_element_type=F32)
        gate, up = both[:, 0:128], both[:, 128:256]
        hidden = gate / (1.0 + jnp.exp(-gate)) * up
        turn = (u - S0 + SLOT_UNITS - TURN) % SLOT_UNITS
        ring[y, x, pl.ds((turn + H0) * UNIT, UNIT), :] = hidden.astype(BF)

    def pooled_unit(u):
        out[pl.ds((u - P0) * UNIT, UNIT), :] = jnp.dot(
            wide(u), w_mix[...], preferred_element_type=F32
        ).astype(BF)

    def hidden_unit(u):
        turn = (u - H0 + TURN) % SLOT_UNITS
        back[pl.ds(turn * UNIT, UNIT), :] = jnp.dot(
            wide(u), w_down[...], preferred_element_type=F32
        ).astype(BF)

    def halo_out():
        remote(
            inner.at[rows - 16 : rows],
            halo.at[0:16],
            halo_send,
            halo_sem.at[0],
            {"ep": (ep + 1) % n_ep},
        )
        remote(
            inner.at[0:16],
            halo.at[16:32],
            halo_send,
            halo_sem.at[1],
            {"ep": (ep + n_ep - 1) % n_ep},
        )

    def pool():
        await_bytes(halo.at[0:16], halo_sem.at[0])
        await_bytes(halo.at[16:32], halo_sem.at[1])
        low = jnp.where(ep > 0, halo[8:16, :].astype(F32), 0.0)
        high = jnp.where(ep < n_ep - 1, halo[16:24, :].astype(F32), 0.0)
        values = inner[...].astype(F32)
        ext = jnp.concatenate([low, values, high], axis=0)
        two = ext[0 : rows + 15, :] + ext[1 : rows + 16, :]
        four = two[0 : rows + 13, :] + two[2 : rows + 15, :]
        eight = four[0 : rows + 9, :] + four[4 : rows + 13, :]
        sixteen = eight[0 : rows + 1, :] + eight[8 : rows + 9, :]
        total = jnp.where(
            y == 0,
            two[7 : 7 + rows, :],
            jnp.where(
                y == 1,
                four[6 : 6 + rows, :],
                jnp.where(y == 2, eight[4 : 4 + rows, :], sixteen[0:rows, :]),
            ),
        )
        reach = jnp.where(y == 0, 1, jnp.where(y == 1, 2, jnp.where(y == 2, 4, 8)))
        token = ep * rows + lax.broadcasted_iota(jnp.int32, (rows, 128), 0)
        count = jnp.minimum(token + reach, n_ep * rows) - jnp.maximum(token - reach, 0)
        result = (total / count.astype(F32) - values) * scale_ref[...]
        ring[y, x, P0 * UNIT : P0 * UNIT + rows, :] = result.astype(BF)

    def send_back(g):
        for q in range(8 * g, 8 * g + 8):
            part = slice(q * CAP, (q + 1) * CAP)
            if q == 0:
                returned[part, :] = back[part, :]
            else:
                remote(
                    back.at[part], returned.at[part], back_send, back_sem.at[g], peer_at(q, -1)
                )

    group = 8 * CAP
    lane = lax.broadcasted_iota(jnp.int32, (2 * rows, 128), 1).astype(F32)

    def combine(g):
        count = group if g > 0 else group - CAP
        await_bytes(returned.at[0:count], back_sem.at[g])
        where = slot_of[...]
        hot = jnp.concatenate(
            [
                jnp.where(where == lane + float(g * group + c * 128), 1.0, 0.0).astype(BF)
                for c in range(group // 128)
            ],
            axis=1,
        )
        picked[...] += jnp.dot(
            hot, returned[g * group : (g + 1) * group, :], preferred_element_type=F32
        )

    n_groups = n_ep // 8

    def sends(u):
        return ((u >= M0) & (u < M0 + rows // UNIT)) | ((u >= S0) & (u < UNITS))

    def step(i, carry):
        for lag, stage in ((B2, second_b), (B1, first_b), (A2, second_a)):
            u = i - lag

            @pl.when((u >= S0) & (u < UNITS) if stage is second_a else sends(u))
            def _():
                stage(u)

        k = i - S0
        for first, count in ((0, 3), (1, 3), (2, 2)):

            @pl.when((k > 0) & (k < SLOT_UNITS) & (k % 3 == first))
            def _():
                await_bytes(ring.at[y, x, 0 : count * CAP], disp_sem.at[k])

        @pl.when(k == 0)
        def _():
            await_bytes(ring.at[y, x, 0 : 2 * CAP], disp_sem.at[0])

        @pl.when((i >= S0) & (i < UNITS))
        def _():
            first_a(i)

        u = i - DONE

        @pl.when(u == UNITS - 2)
        def _():
            combine(0)
            out[rows : 2 * rows, :] = (
                picked[0:rows, :] * weight_of[0:rows, :]
                + picked[rows : 2 * rows, :] * weight_of[rows : 2 * rows, :]
            ).astype(BF)

        @pl.when(sends(u))
        def _():
            finished(u)

        @pl.when(u == S0 + 2)
        def _():
            place_results()

        @pl.when(u == M0)
        def _():
            for copy in weights:
                copy.wait()

        @pl.when((u >= M0) & (u < M0 + rows // UNIT))
        def _():
            mixer_unit(u)

        @pl.when(u == M0 + rows // UNIT - 1)
        def _():
            halo_out()

        @pl.when(u == M0 + rows // UNIT + 2)
        def _():
            pool()

        @pl.when((u >= S0) & (u < H0))
        def _():
            slot_unit(u)

        @pl.when(u >= P0)
        def _():
            pooled_unit(u)

        @pl.when((u >= H0) & (u < P0))
        def _():
            hidden_unit(u)

        for g in range(n_groups):

            @pl.when(u == H0 + 3 * g + 2)
            def _():
                if g > 0:
                    combine(g)
                send_back((g + 1) % n_groups)

        return carry

    lax.fori_loop(B1, UNITS + DONE, step, 0)
    sent = (SIDE * SIDE - 1) * (2 * rows + 2 * slots) // (SIDE * SIDE)
    await_bytes(ring.at[:, :, 0:sent], send_sem)
    await_bytes(outgoing.at[0 : slots - CAP], disp_send)
    await_bytes(back.at[0 : slots - CAP], back_send)
    await_bytes(inner.at[0:32], halo_send)


def on_device(
    mixer_rows,
    expert_rows,
    mixer_gain,
    pool_scale,
    w_in,
    w_mix_out,
    expert_gain,
    expert_gate,
    expert_up,
    expert_down,
    routes,
    route_weight,
):
    rows, feats = mixer_rows.shape
    n_ep = lax.axis_size("ep")
    depth = w_in.shape[0]
    vmem = pl.BlockSpec(memory_space=pltpu.VMEM)
    hbm = pl.BlockSpec(memory_space=pl.ANY)
    slots = n_ep * CAP
    both = pl.pallas_call(
        kernel,
        name="mixer_and_experts",
        out_shape=jax.ShapeDtypeStruct((2 * rows, feats), BF),
        in_specs=[hbm] * 12,
        out_specs=vmem,
        scratch_shapes=[
            pltpu.VMEM((SIDE, SIDE, UNITS * UNIT, feats), BF),
            pltpu.VMEM((depth, 128), BF),
            pltpu.VMEM((depth, 128), BF),
            pltpu.VMEM((depth, 256), BF),
            pltpu.VMEM((depth, 128), BF),
            pltpu.VMEM((slots, feats), BF),
            pltpu.VMEM((slots, feats), BF),
            pltpu.VMEM((slots, feats), BF),
            pltpu.VMEM((UNIT, depth), BF),
            pltpu.VMEM((rows, feats), BF),
            pltpu.VMEM((32, feats), BF),
            pltpu.VMEM((2 * rows, 128), F32),
            pltpu.VMEM((2 * rows, 128), F32),
            pltpu.VMEM((n_ep, rows), F32),
            pltpu.VMEM((2 * rows, feats), F32),
            pltpu.VMEM((rows, feats), BF),
            pltpu.VMEM((depth // 128, 128), F32),
            pltpu.VMEM((1, feats), F32),
            pltpu.VMEM((depth // 128, 128), F32),
            pltpu.VMEM((2, rows), jnp.int32),
            pltpu.VMEM((2, rows), F32),
            pltpu.SemaphoreType.DMA((5,)),
            pltpu.SemaphoreType.DMA((7,)),
            pltpu.SemaphoreType.DMA,
            pltpu.SemaphoreType.DMA((UNITS, 2, 4)),
            pltpu.SemaphoreType.DMA,
            pltpu.SemaphoreType.DMA((SLOT_UNITS,)),
            pltpu.SemaphoreType.DMA,
            pltpu.SemaphoreType.DMA((n_ep // 8,)),
            pltpu.SemaphoreType.DMA,
            pltpu.SemaphoreType.DMA((2,)),
        ],
        compiler_params=pltpu.CompilerParams(
            collective_id=0, has_side_effects=True, vmem_limit_bytes=60 * 1024 * 1024
        ),
    )(
        mixer_rows,
        expert_rows,
        mixer_gain.reshape(-1, 128),
        pool_scale.reshape(1, -1),
        expert_gain.reshape(-1, 128),
        routes.T,
        route_weight.T,
        w_in,
        w_mix_out,
        expert_gate[0],
        expert_up[0],
        expert_down[0],
    )
    return both[0:rows], both[rows:]


def solution(mesh):
    return jax.shard_map(
        on_device,
        mesh=mesh,
        in_specs=(
            P("ep", "tp"),
            P("ep", "tp"),
            P(),
            P("tp"),
            P(None, "tp"),
            P(None, "tp"),
            P(),
            P("ep", None, "tp"),
            P("ep", None, "tp"),
            P("ep", None, "tp"),
            P("ep", None),
            P("ep", None),
        ),
        out_specs=(P("ep", "tp"), P("ep", "tp")),
        check_vma=False,
    )
```
